32 devices in a mesh: ep: 8 (over z, x), tp: 4 (over y, core).
Axes of the slice: x: 2, y: 2, z: 4, core: 2. Of those that a mesh axis runs over, the one named last changes fastest.
Arguments:
- mixer_input: bfloat16 [4096, 2048], P('ep'), may hold values from -5.5 to 5.5
- expert_input: bfloat16 [4096, 2048], P('ep'), may hold values from -6 to 6
- gain_mixer: float32 [2048], replicated, may hold values from 0.1 to 1.9
- gain_expert: float32 [2048], replicated, may hold values from 0.1 to 1.9
- query_weight: bfloat16 [2048, 1536], P(None, 'tp')
- key_weight: bfloat16 [2048, 256], P(None, 'tp')
- value_weight: bfloat16 [2048, 256], P(None, 'tp'), may hold values from -0.125 to 0.125
- sink_logits: float32 [24], P('tp'), may hold values from 2 to 6
- output_weight: bfloat16 [1536, 2048], P('tp'), may hold values from -0.75 to 0.75
- expert_choice: int32 [4096, 2], P('ep'), may hold values from 0 to 7, all different within a row; in each aligned block of 128 rows (0 to 127, 128 to 255, ...) at most 64 rows name the same one
- route_weights: float32 [4096, 2], P('ep'), may hold values from 0.2 to 1.2
- expert_gate: bfloat16 [8, 2048, 1024], P('ep', None, 'tp'), may hold values from -0.125 to 0.125
- expert_up: bfloat16 [8, 2048, 1024], P('ep', None, 'tp'), may hold values from -0.125 to 0.125
- expert_down: bfloat16 [8, 1024, 2048], P('ep', 'tp'), may hold values from -0.1875 to 0.1875
- shared_gate: bfloat16 [2048, 512], P(None, 'tp'), may hold values from -0.125 to 0.125
- shared_up: bfloat16 [2048, 512], P(None, 'tp'), may hold values from -0.125 to 0.125
- shared_down: bfloat16 [512, 2048], P('tp'), may hold values from -0.25 to 0.25
Outputs:
- mixer_output: bfloat16 [4096, 2048], P(('ep', 'tp'))
- expert_output: bfloat16 [4096, 2048], P(('ep', 'tp'))
The draws below stay inside these ranges and needn't reach their ends.
Inputs may be any that keep to these rules, and one draw needn't show every extreme that they name: `expert_choice`: in each aligned block of 128 rows no expert is named by more than 64 rows, and in some block some expert is named by exactly 64 rows; the 2 entries of a row differ.
All inputs are finite; a program needn't handle non-finite values.
Results may differ from the reference program's by a relative error of at most 0.019.
Values may be sent and summed in bfloat16 or wider, within the bound.
A program may use at most 128 MiB of HBM per device.

```python
import math
import jax
import jax.numpy as jnp
import numpy as np
from jax import lax

D = 2048
HEADS = 24
KV_HEADS = 4
HEAD_DIM = 64
WINDOW = 128
SEQS = 1
EXPERT_FF = 1024
SHARED_FF = 512
TOP = 2
TOK_B_DEV = 128
EXPERTS = 8
TOKENS_A = 4096
TOKENS_B = 4096
SEQ_LEN = 4096
CAP = 64
N_TP = 4


def attention_weights(key):
    base_key = jax.random.fold_in(key, 41)
    key_part = jax.random.truncated_normal(jax.random.fold_in(base_key, 1), -4.0, 4.0, (D, KV_HEADS * HEAD_DIM), jnp.float32) * D ** (-0.5)
    query_part = jax.random.truncated_normal(jax.random.fold_in(base_key, 2), -4.0, 4.0, (D, HEADS * HEAD_DIM), jnp.float32) * D ** (-0.5)
    return (key_part, query_part)


def draw_key_weight(key, part):
    key_part, query_part = attention_weights(key)
    return key_part.astype(jnp.bfloat16)


def draw_query_weight(key, part):
    key_part, query_part = attention_weights(key)
    return query_part.astype(jnp.bfloat16)


def draw_mixer_input(key, part):
    base_key = jax.random.fold_in(key, 53)
    values = jax.random.truncated_normal(jax.random.fold_in(base_key, 1), -5.0, 5.0, (TOKENS_A, D), jnp.float32)
    return values.astype(jnp.bfloat16)


def steps_of(stream_key, dims, pieces, low, largest):
    def one(axis_at, parts):
        draws = jax.random.uniform(jax.random.fold_in(jax.random.fold_in(stream_key, 6), axis_at), (parts,), jnp.float32, low / len(pieces), largest / len(pieces))
        return jnp.repeat(jnp.exp(draws), dims[axis_at] // parts).reshape((-1,) + (1,) * (len(dims) - axis_at - 1))

    loudness = one(*pieces[0])
    for cut in pieces[1:]:
        loudness = loudness * one(*cut)
    return loudness


def deal_out(stream_key, own, number, rows, amount, top, most, lean):
    ranking = jax.random.permutation(stream_key, amount)
    crowded, ordinary = shares(amount, rows * top, most, lean, True), shares(amount, rows * top, most, lean, False)
    places = jnp.arange(amount)

    def named(tallies, turn):
        used = int((tallies > 0).sum())
        fixed = max(1, used // 4)
        moved = fixed + (places - fixed + turn * (used - fixed)) % max(1, amount - fixed)
        return jnp.zeros((amount,), jnp.int32).at[ranking[jnp.where(places < fixed, places, moved)]].set(jnp.asarray(tallies, jnp.int32))

    tallies = jnp.where(number % 4 == 0, named(crowded, number // 4), named(ordinary, number - number // 4 - 1))
    mixed = jax.random.permutation(jax.random.fold_in(own, 3), amount)
    source_of, sink = mixed[0:amount // 2 * 2:2], mixed[1:amount // 2 * 2:2]
    margin = jnp.minimum(tallies[source_of] - 1, most - tallies[sink]) // 2
    margin = jnp.where((source_of == ranking[0]) | (sink == ranking[0]) | (tallies[sink] == 0), 0, jnp.maximum(margin, 0))
    moved = jax.random.randint(jax.random.fold_in(own, 4), (amount // 2,), 0, 1 << 20) % (margin + 1)
    tallies = tallies.at[source_of].add(-moved).at[sink].add(moved)
    items = jnp.searchsorted(jnp.cumsum(tallies), jnp.arange(rows * top), side="right").astype(jnp.int32)
    listing = items.reshape(top, rows).T
    listing = listing[jax.random.permutation(jax.random.fold_in(own, 1), rows)]
    turn = jax.random.randint(jax.random.fold_in(own, 2), (rows, 1), 0, top)
    return jnp.take_along_axis(listing, (jnp.arange(top)[None, :] + turn) % top, axis=1)


def shares(number_of, total, bound, skew, full):
    loads = [(1 << 20) // math.isqrt(grade ** skew) + 1 for grade in range(1, number_of + 1)]
    largest = bound if full else min(bound, max(-(-total // number_of), total * loads[0] // sum(loads)))
    least = 1 if total - largest >= number_of - 1 else 0
    counts, surplus = [largest] + [least] * (number_of - 1), total - largest - least * (number_of - 1)
    while surplus > 0:
        movable = [i for i in range(1, number_of) if counts[i] < largest] or [i for i in range(1, number_of) if counts[i] < bound]
        whole, remaining = sum([loads[i] for i in movable]), surplus
        for i in movable:
            more = min(bound - counts[i], max(1, remaining * loads[i] // whole), surplus)
            counts[i] = counts[i] + more
            surplus = surplus - more
    return np.array(counts)


def bell_draw(own_key, dims, scale, bound, pieces=(), kind=jnp.bfloat16):
    entries = jax.random.normal(own_key, dims, jnp.float32) * scale
    if len(pieces) > 0:
        entries = steps_of(own_key, dims, pieces, -0.22, 0.18) * entries
    return jnp.clip(entries, min=-bound, max=bound).astype(kind)


def setup_inputs(seed: int = 0) -> dict:
    key_of = jax.random.split(jax.random.key(seed), 18)
    mixer_input = draw_mixer_input(jax.random.fold_in(key_of[17], 71), 0)
    expert_input = bell_draw(key_of[1], (TOKENS_B, D), 1.0, 6.0, ((0, 8),))
    gain_mixer = jnp.clip(1.0 + 0.18 * jax.random.normal(key_of[2], (D,), jnp.float32), 0.1, 1.9)
    gain_expert = jnp.clip(1.0 + 0.18 * jax.random.normal(key_of[3], (D,), jnp.float32), 0.1, 1.9)
    query_weight = draw_query_weight(jax.random.fold_in(key_of[17], 71), 0)
    key_weight = draw_key_weight(jax.random.fold_in(key_of[17], 71), 0)
    value_weight = bell_draw(key_of[6], (D, KV_HEADS * HEAD_DIM), D ** -0.5, 0.125, ((1, 4),))
    sink_logits = jnp.clip(2.0 + 4.0 * jax.random.uniform(key_of[7], (HEADS,), jnp.float32) ** steps_of(key_of[7], (HEADS,), ((0, 4),), -0.2, 0.2), 2.0, 6.0)
    output_weight = bell_draw(key_of[8], (HEADS * HEAD_DIM, D), (HEADS * HEAD_DIM // 25) ** -0.5, 0.75, ((0, 4),))
    expert_choice_keys = jax.random.split(jax.random.fold_in(key_of[9], 1), TOKENS_B // TOK_B_DEV)
    expert_choice_turns = jax.random.permutation(jax.random.fold_in(key_of[9], 3), TOKENS_B // TOK_B_DEV)
    expert_choice = jax.vmap(lambda own, number: deal_out(jax.random.fold_in(key_of[9], 2), own, number, TOK_B_DEV, EXPERTS, TOP, CAP, 2))(expert_choice_keys, expert_choice_turns).reshape((TOKENS_B, TOP))
    route_weights = jnp.clip(0.2 + 1 * jax.random.uniform(key_of[10], (TOKENS_B, TOP), jnp.float32) ** steps_of(key_of[10], (TOKENS_B, TOP), ((0, 8),), -0.2, 0.2), 0.2, 1.2)
    expert_gate = bell_draw(key_of[11], (EXPERTS, D, EXPERT_FF), D ** -0.5, 0.125, ((0, 8), (2, 4)))
    expert_up = bell_draw(key_of[12], (EXPERTS, D, EXPERT_FF), D ** -0.5, 0.125, ((0, 8), (2, 4)))
    expert_down = bell_draw(key_of[13], (EXPERTS, EXPERT_FF, D), EXPERT_FF ** -0.5, 0.1875, ((0, 8), (1, 4)))
    shared_gate = bell_draw(key_of[14], (D, SHARED_FF), D ** -0.5, 0.125, ((1, 4),))
    shared_up = bell_draw(key_of[15], (D, SHARED_FF), D ** -0.5, 0.125, ((1, 4),))
    shared_down = bell_draw(key_of[16], (SHARED_FF, D), SHARED_FF ** -0.5, 0.25, ((0, 4),))
    return dict(mixer_input=mixer_input, expert_input=expert_input, gain_mixer=gain_mixer, gain_expert=gain_expert, query_weight=query_weight, key_weight=key_weight, value_weight=value_weight, sink_logits=sink_logits, output_weight=output_weight, expert_choice=expert_choice, route_weights=route_weights, expert_gate=expert_gate, expert_up=expert_up, expert_down=expert_down, shared_gate=shared_gate, shared_up=shared_up, shared_down=shared_down)


norm_eps = 1e-06
rope_base = 500000.0

def rounded(value):
    return lax.optimization_barrier(value.astype(jnp.bfloat16)).astype(jnp.float32)

def rms_scale(matrix, scaling):
    widened = matrix.astype(jnp.float32)
    scaled = widened * lax.rsqrt(lax.optimization_barrier(jnp.mean(widened * widened, axis=-1, keepdims=True)) + norm_eps)
    return (scaled * scaling).astype(jnp.bfloat16)

def frequencies(head_size):
    half_steps = jnp.arange(head_size // 2, dtype=jnp.float32)
    return rope_base ** (-(2.0 * half_steps) / head_size)

def rotate(heads, angles):
    middle = heads.shape[-1] // 2
    widened = heads.astype(jnp.float32)
    cosine = jnp.cos(angles)[:, None, :]
    sine_val = jnp.sin(angles)[:, None, :]
    leading = widened[..., :middle]
    trailing = widened[..., middle:]
    turned = jnp.concatenate([leading * cosine - trailing * sine_val, trailing * cosine + leading * sine_val], axis=-1)
    return turned.astype(jnp.bfloat16)

def attend(query_heads, key_heads, value_heads, prior_keys, prior_values, first_position, sink_logits):
    window = prior_keys.shape[0]
    total_rows, kv_count, head_size = key_heads.shape
    group_size = query_heads.shape[1] // kv_count
    blocks = total_rows // window

    def banded(earlier, current):
        joined = jnp.concatenate([earlier, current], axis=0).reshape(blocks + 1, window, kv_count, head_size)
        return jnp.concatenate([joined[:-1], joined[1:]], axis=1)
    band_keys = banded(prior_keys, key_heads)
    band_values = banded(prior_values, value_heads)
    query_blocks = query_heads.reshape(blocks, window, kv_count, group_size, head_size)
    scores = jnp.einsum('nqhgd,nkhd->nhgqk', query_blocks.astype(jnp.float32), band_keys.astype(jnp.float32)) / math.sqrt(head_size)
    query_index = jnp.arange(window, dtype=jnp.int32)[:, None]
    key_index = jnp.arange(2 * window, dtype=jnp.int32)[None, :]
    distance = query_index + window - key_index
    block_start = first_position + jnp.arange(blocks, dtype=jnp.int32)[:, None, None] * window
    allowed = (distance >= 0) & (distance < window) & (block_start - window + key_index >= 0)
    scores = jnp.where(allowed[:, None, None, :, :], scores, -jnp.inf)
    sink_grid = sink_logits.astype(jnp.float32).reshape(kv_count, group_size)[None, :, :, None, None]
    row_peak = jnp.maximum(lax.optimization_barrier(jnp.max(scores, axis=-1, keepdims=True)), sink_grid)
    shifted_exp = jnp.exp(scores - row_peak)
    denominator = lax.optimization_barrier(jnp.sum(shifted_exp, axis=-1, keepdims=True)) + jnp.exp(sink_grid - row_peak)
    probs = (shifted_exp / denominator).astype(jnp.bfloat16)
    attended = jnp.einsum('nhgqk,nkhd->nqhgd', probs.astype(jnp.float32), band_values.astype(jnp.float32))
    return attended.astype(jnp.bfloat16).reshape(total_rows, kv_count * group_size * head_size)

def reference(mixer_input, expert_input, gain_mixer, gain_expert, query_weight, key_weight, value_weight, sink_logits, output_weight, expert_choice, route_weights, expert_gate, expert_up, expert_down, shared_gate, shared_up, shared_down):
    head_block = HEADS * HEAD_DIM // N_TP

    def one_sequence(seq_rows):
        normed = rms_scale(seq_rows, gain_mixer)
        queries = jnp.dot(normed, query_weight, preferred_element_type=jnp.float32).astype(jnp.bfloat16)
        key_rows = jnp.dot(normed, key_weight, preferred_element_type=jnp.float32).astype(jnp.bfloat16)
        value_rows = jnp.dot(normed, value_weight, preferred_element_type=jnp.float32).astype(jnp.bfloat16)
        positions = jnp.arange(SEQ_LEN, dtype=jnp.float32)
        angles = positions[:, None] * frequencies(HEAD_DIM)[None, :]
        rot_queries = rotate(queries.reshape(SEQ_LEN, HEADS, HEAD_DIM), angles)
        rot_keys = rotate(key_rows.reshape(SEQ_LEN, KV_HEADS, HEAD_DIM), angles)
        value_heads = value_rows.reshape(SEQ_LEN, KV_HEADS, HEAD_DIM)
        empty_rows = jnp.zeros((WINDOW, KV_HEADS, HEAD_DIM), jnp.bfloat16)
        attended = attend(rot_queries, rot_keys, value_heads, empty_rows, empty_rows, 0, sink_logits)
        mixed_sum = jnp.zeros((SEQ_LEN, D), jnp.float32)
        for slice_index in range(N_TP):
            low_edge = slice_index * head_block
            mixed_sum = mixed_sum + rounded(jnp.dot(attended[:, low_edge:low_edge + head_block], output_weight[low_edge:low_edge + head_block], preferred_element_type=jnp.float32))
        return mixed_sum.astype(jnp.bfloat16)
    mixer_output = lax.map(one_sequence, mixer_input.reshape(SEQS, SEQ_LEN, D)).reshape(TOKENS_A, D)
    normed_rows = rms_scale(expert_input, gain_expert)
    padded_rows = jnp.concatenate([normed_rows, jnp.zeros((1, D), jnp.bfloat16)], axis=0)
    block_count = TOKENS_B // TOK_B_DEV
    assigned = TOK_B_DEV * TOP
    picked_experts = expert_choice.reshape(block_count, assigned)
    onehot = (picked_experts[:, :, None] == jnp.arange(EXPERTS, dtype=jnp.int32)[None, None, :]).astype(jnp.int32)
    slot_ranks = lax.optimization_barrier(jnp.sum(jnp.cumsum(onehot, axis=1) * onehot, axis=-1)) - 1
    block_ids = jnp.arange(block_count, dtype=jnp.int32)[:, None]
    slot_index = (picked_experts * block_count + block_ids) * CAP + slot_ranks
    token_owner = block_ids * TOK_B_DEV + jnp.arange(assigned, dtype=jnp.int32)[None, :] // TOP
    slot_table = jnp.full((EXPERTS * block_count * CAP,), TOKENS_B, jnp.int32).at[slot_index.reshape(-1)].set(token_owner.reshape(-1).astype(jnp.int32))
    weight_table = jnp.zeros((EXPERTS * block_count * CAP,), jnp.float32).at[slot_index.reshape(-1)].set(route_weights.reshape(-1).astype(jnp.float32))
    ff_block = EXPERT_FF // N_TP

    def one_expert(carry, inputs):
        index_row, weight_row, gate_matrix, up_matrix, down_matrix = inputs
        chosen_rows = padded_rows[index_row]
        gate_values = jnp.dot(chosen_rows, gate_matrix, preferred_element_type=jnp.float32)
        up_values = jnp.dot(chosen_rows, up_matrix, preferred_element_type=jnp.float32)
        hidden = (jax.nn.silu(gate_values) * up_values).astype(jnp.bfloat16)
        result = jnp.zeros((chosen_rows.shape[0], D), jnp.float32)
        for slice_index in range(N_TP):
            low_edge = slice_index * ff_block
            result = result + rounded(jnp.dot(hidden[:, low_edge:low_edge + ff_block], down_matrix[low_edge:low_edge + ff_block], preferred_element_type=jnp.float32))
        return (carry.at[index_row].add(result * weight_row[:, None]), None)
    routed, unused = lax.scan(one_expert, jnp.zeros((TOKENS_B + 1, D), jnp.float32), (slot_table.reshape(EXPERTS, block_count * CAP), weight_table.reshape(EXPERTS, block_count * CAP), expert_gate, expert_up, expert_down))
    shared_gate_values = jnp.dot(normed_rows, shared_gate, preferred_element_type=jnp.float32)
    shared_up_values = jnp.dot(normed_rows, shared_up, preferred_element_type=jnp.float32)
    shared_hidden = (jax.nn.silu(shared_gate_values) * shared_up_values).astype(jnp.bfloat16)
    shared_block = SHARED_FF // N_TP
    shared_result = jnp.zeros((TOKENS_B, D), jnp.float32)
    for slice_index in range(N_TP):
        low_edge = slice_index * shared_block
        shared_result = shared_result + rounded(jnp.dot(shared_hidden[:, low_edge:low_edge + shared_block], shared_down[low_edge:low_edge + shared_block], preferred_element_type=jnp.float32))
    expert_output = (routed[:TOKENS_B] + shared_result).astype(jnp.bfloat16)
    return (mixer_output, expert_output)
```

```python
import functools
import math

import jax
import jax.numpy as jnp
from jax import lax
from jax.experimental import pallas as pl
from jax.experimental.pallas import tpu as pltpu
from jax.sharding import PartitionSpec as P

HEAD_DIM = 64
WINDOW = 128
SEQS = 1
PIECES = 4


norm_eps = 1e-06
rope_base = 500000.0
bf16 = jnp.bfloat16
f32 = jnp.float32
MESH = pl.DeviceIdType.MESH


def from_behind(value, axis, steps):
    count = lax.axis_size(axis)
    first, last = (max(0, -steps), min(count, count - steps))
    return lax.ppermute(value, axis, [(source, source + steps) for source in range(first, last)])


def rms_scale(matrix, scaling):
    widened = matrix.astype(jnp.float32)
    scaled = widened * lax.rsqrt(jnp.mean(widened * widened, axis=-1, keepdims=True) + norm_eps)
    return (scaled * scaling).astype(jnp.bfloat16)


def frequencies(head_size):
    half_steps = jnp.arange(head_size // 2, dtype=jnp.float32)
    return rope_base ** (-(2.0 * half_steps) / head_size)


def rotate(heads, angles):
    middle = heads.shape[-1] // 2
    widened = heads.astype(jnp.float32)
    cosine = jnp.cos(angles)[:, None, :]
    sine_val = jnp.sin(angles)[:, None, :]
    leading = widened[..., :middle]
    trailing = widened[..., middle:]
    turned = jnp.concatenate(
        [leading * cosine - trailing * sine_val, trailing * cosine + leading * sine_val], axis=-1
    )
    return turned.astype(jnp.bfloat16)


def attend(
    query_heads, key_heads, value_heads, prior_keys, prior_values, first_position, sink_logits
):
    window = prior_keys.shape[0]
    total_rows, kv_count, head_size = key_heads.shape
    group_size = query_heads.shape[1] // kv_count
    blocks = total_rows // window

    def banded(earlier, current):
        joined = jnp.concatenate([earlier, current], axis=0).reshape(
            blocks + 1, window, kv_count, head_size
        )
        return jnp.concatenate([joined[:-1], joined[1:]], axis=1)

    band_keys = banded(prior_keys, key_heads)
    band_values = banded(prior_values, value_heads)
    query_blocks = query_heads.reshape(blocks, window, kv_count, group_size, head_size)
    scores = jnp.einsum(
        "nqhgd,nkhd->nhgqk", query_blocks, band_keys, preferred_element_type=jnp.float32
    ) / math.sqrt(head_size)
    query_index = jnp.arange(window, dtype=jnp.int32)[:, None]
    key_index = jnp.arange(2 * window, dtype=jnp.int32)[None, :]
    distance = query_index + window - key_index
    block_start = first_position + jnp.arange(blocks, dtype=jnp.int32)[:, None, None] * window
    allowed = (distance >= 0) & (distance < window) & (block_start - window + key_index >= 0)
    scores = jnp.where(allowed[:, None, None, :, :], scores, -jnp.inf)
    sink_grid = sink_logits.reshape(kv_count, group_size)[None, :, :, None, None]
    row_peak = jnp.maximum(jnp.max(scores, axis=-1, keepdims=True), sink_grid)
    shifted_exp = jnp.exp(scores - row_peak)
    denominator = jnp.sum(shifted_exp, axis=-1, keepdims=True) + jnp.exp(sink_grid - row_peak)
    probs = (shifted_exp / denominator).astype(jnp.bfloat16)
    attended = jnp.einsum(
        "nhgqk,nkhd->nqhgd", probs, band_values, preferred_element_type=jnp.float32
    )
    return attended.astype(jnp.bfloat16).reshape(total_rows, kv_count * group_size * head_size)


def rows_at(start, count, unit):
    return pl.ds(pl.multiple_of(start, unit), count)


def norm_into(target, source, start, count, gain):
    step = 32

    def body(i, carry):
        widened = source[rows_at(start + i * step, step, step), :].astype(f32)
        scale = lax.rsqrt(jnp.mean(widened * widened, axis=-1, keepdims=True) + norm_eps)
        target[rows_at(i * step, step, step), :] = (widened * scale * gain[...]).astype(bf16)
        return carry

    lax.fori_loop(0, count // step, body, 0)


def silu_times(gate, up):
    return gate / (1.0 + jnp.exp(-gate)) * up


def mixture_kernel(
    capacity,
    x_ref, part_ref, gain_ref, choice_ref, route_ref,
    wg_ref, wu_ref, wd_ref, sg_ref, su_ref, sd_ref,
    mixer_out, expert_out,
    rows_in, normed, gain, choice, route, wg, wu, wd, sg, su, sd,
    own_rows, slots_out, slots_in, hidden, result, back, picks, weights_col,
    mixer_part, shared_part, shared_hidden, half_in, half_out, last_in,
    load_sem, far_send, far_recv, mate_send, mate_recv, pass_send, pass_recv,
    slot_send, slot_recv, back_send, back_recv, half_send, half_recv, last_send, last_recv,
):
    ep_count = lax.axis_size("ep")
    me = lax.axis_index("ep")
    t = lax.axis_index("tp")
    parity = t % 2
    level = t // 2
    mate = t + 1 - 2 * parity
    far = (t + 2) % 4
    far_mate = (mate + 2) % 4
    tokens, width = rows_in.shape
    own = own_rows.shape[0]
    ff = wd_ref.shape[0]
    slots = slots_out.shape[0]
    piece = width // PIECES

    barrier = pltpu.get_barrier_semaphore()

    def greet(k, carry):
        pl.semaphore_signal(barrier, inc=1, device_id={"ep": (me + k) % ep_count}, device_id_type=MESH)
        return carry

    lax.fori_loop(1, ep_count, greet, 0)
    for other in (mate, far):
        pl.semaphore_signal(barrier, inc=1, device_id={"tp": other}, device_id_type=MESH)

    loads = [
        (gain_ref, gain), (choice_ref, choice), (route_ref, route), (x_ref, rows_in),
        (wg_ref, wg.at[t]), (wu_ref, wu.at[t]), (wd_ref, wd.at[rows_at(t * ff, ff, ff)]),
        (sg_ref, sg), (su_ref, su), (sd_ref, sd), (part_ref, mixer_part),
    ]
    loads = [pltpu.make_async_copy(a, b, load_sem.at[i]) for i, (a, b) in enumerate(loads)]
    for load in loads:
        load.start()

    pl.semaphore_wait(barrier, ep_count + 1)

    def block_views(owner):
        views = [wg.at[owner], wu.at[owner]]
        down = wd.at[rows_at(owner * ff, ff, ff)]
        return views + [down.at[:, pl.ds(c * piece, piece)] for c in range(PIECES)]

    sources = [wg_ref, wu_ref] + [wd_ref.at[:, pl.ds(c * piece, piece)] for c in range(PIECES)]

    def remote(src, dst, send, recv, device):
        return pltpu.make_async_remote_copy(
            src_ref=src, dst_ref=dst, send_sem=send, recv_sem=recv,
            device_id=device, device_id_type=MESH,
        )

    def views_copy(srcs, owner, send, recv, device):
        return [
            remote(a, b, send.at[i], recv.at[i], device)
            for i, (a, b) in enumerate(zip(srcs, block_views(owner)))
        ]

    to_far = views_copy(sources, t, far_send, far_recv, {"tp": far})
    to_mate = views_copy(sources, t, mate_send, mate_recv, {"tp": mate})
    from_far = views_copy(sources, far, far_send, far_recv, {"tp": far})
    from_mate = views_copy(sources, mate, mate_send, mate_recv, {"tp": mate})
    to_pass = views_copy(block_views(far), far, pass_send, pass_recv, {"tp": mate})
    from_pass = views_copy(block_views(far), far_mate, pass_send, pass_recv, {"tp": mate})
    for copy in to_far:
        copy.start()

    for i in (0, 1, 2, 3):
        loads[i].wait()
    norm_into(own_rows, rows_in, t * own, own, gain)
    lanes = rows_at(t * own, own, own)
    top = choice.shape[0]
    chosen = choice[:, lanes]
    row_ids = lax.broadcasted_iota(jnp.int32, (slots // capacity, own), 0)
    named = [row_ids == chosen[k : k + 1, :] for k in range(top)]
    named_any = functools.reduce(jnp.logical_or, named).astype(f32)
    earlier = lax.broadcasted_iota(jnp.int32, (own, own), 0)
    later = lax.broadcasted_iota(jnp.int32, (own, own), 1)
    ranks = jnp.dot(named_any, (earlier < later).astype(f32), preferred_element_type=f32)
    slot_rows = [
        chosen[k : k + 1, :] * capacity
        + jnp.sum(jnp.where(named[k], ranks, 0.0), axis=0, keepdims=True).astype(jnp.int32)
        for k in range(top)
    ]
    slot_ids = lax.broadcasted_iota(jnp.int32, (slots, own), 0)
    spread = functools.reduce(jnp.logical_or, [slot_ids == row for row in slot_rows])
    spread = spread.astype(f32).astype(bf16)
    for c in range(PIECES):
        cols = pl.ds(c * piece, piece)
        slots_out[:, cols] = jnp.dot(spread, own_rows[:, cols], preferred_element_type=f32).astype(bf16)

    def slot_block(ref, owner):
        return ref.at[rows_at(owner * capacity, capacity, capacity)]

    def slot_copy(k, target, origin):
        return remote(
            slot_block(slots_out, target), slot_block(slots_in, origin),
            slot_send.at[k], slot_recv.at[k], {"ep": target},
        )

    def send_slots(k, carry):
        slot_copy(k, (me + k) % ep_count, me).start()
        return carry

    lax.fori_loop(1, ep_count, send_slots, 0)
    for copy in to_mate:
        copy.start()

    own_block = rows_at(me * capacity, capacity, capacity)
    slots_in[own_block, :] = slots_out[own_block, :]
    lane_ids = lax.broadcasted_iota(jnp.int32, (own, slots), 1)
    for k in range(top):
        column = jnp.broadcast_to(slot_rows[k].astype(f32), (own, own)).T[:, :1].astype(jnp.int32)
        picks[k] = (lane_ids == column).astype(f32).astype(bf16)
        weights_col[k] = jnp.broadcast_to(route[k : k + 1, lanes], (own, own)).T

    def half_copy(i, part):
        return remote(
            part.at[1 - parity], half_in.at[i], half_send.at[i], half_recv.at[i], {"tp": mate}
        )

    def last_copy(i):
        return remote(
            half_out.at[i], last_in.at[i], last_send.at[i], last_recv.at[i], {"tp": far}
        )

    def middle(i, part):
        half_copy(i, part).wait_recv()
        half_out[i] = (part[parity, 1 - level].astype(f32) + half_in[i, 1 - level].astype(f32)).astype(bf16)
        last_copy(i).start()

    loads[10].wait()
    half_copy(0, mixer_part).start()

    norm_into(normed, rows_in, 0, tokens, gain)
    for i in (7, 8, 9):
        loads[i].wait()
    for r in range(2):
        rows = pl.ds(r * (tokens // 2), tokens // 2)
        gate = jnp.dot(normed[rows, :], sg[...], preferred_element_type=f32)
        up = jnp.dot(normed[rows, :], su[...], preferred_element_type=f32)
        shared_hidden[rows, :] = silu_times(gate, up).astype(bf16)
    for owner in range(4):
        for c in range(PIECES):
            cols = pl.ds(c * piece, piece)
            shared_part[owner % 2, owner // 2, :, cols] = jnp.dot(
                shared_hidden[pl.ds(owner * own, own), :], sd[:, cols], preferred_element_type=f32
            ).astype(bf16)
    half_copy(1, shared_part).start()
    middle(0, mixer_part)
    middle(1, shared_part)

    def hidden_block(owner):
        step = 256
        columns = rows_at(owner * ff, ff, ff)

        def body(i, carry):
            rows = rows_at(i * step, step, step)
            gate = jnp.dot(slots_in[rows, :], wg[owner], preferred_element_type=f32)
            up = jnp.dot(slots_in[rows, :], wu[owner], preferred_element_type=f32)
            hidden[rows, columns] = silu_times(gate, up).astype(bf16)
            return carry

        lax.fori_loop(0, slots // step, body, 0)

    from_far[0].wait_recv()
    to_pass[0].start()

    def wait_slots(k, carry):
        slot_copy(k, me, (me + ep_count - k) % ep_count).wait_recv()
        return carry

    lax.fori_loop(1, ep_count, wait_slots, 0)
    for i in (4, 5, 6):
        loads[i].wait()
    hidden_block(t)
    for copy in from_mate:
        copy.wait_recv()
    hidden_block(mate)
    from_far[1].wait_recv()
    to_pass[1].start()
    hidden_block(far)
    for i in (0, 1):
        from_pass[i].wait_recv()
    hidden_block(far_mate)

    def back_copy(k, c, target, origin):
        cols = pl.ds(c * piece, piece)
        return remote(
            slot_block(result, target).at[:, cols], slot_block(back, origin).at[:, cols],
            back_send.at[k, c], back_recv.at[k, c], {"ep": target},
        )

    for c in range(PIECES):
        cols = pl.ds(c * piece, piece)
        from_far[2 + c].wait_recv()
        to_pass[2 + c].start()
        from_pass[2 + c].wait_recv()
        step = 256

        def down(i, carry, cols=cols):
            rows = rows_at(i * step, step, step)
            result[rows, cols] = jnp.dot(
                hidden[rows, :], wd[:, cols], preferred_element_type=f32
            ).astype(bf16)
            return carry

        lax.fori_loop(0, slots // step, down, 0)

        def send_back(k, carry, c=c):
            back_copy(k, c, (me + k) % ep_count, me).start()
            return carry

        lax.fori_loop(1, ep_count, send_back, 0)
        back[own_block, cols] = result[own_block, cols]

    def summed(i, part):
        return part[parity, level].astype(f32) + half_in[i, level].astype(f32) + last_in[i].astype(f32)

    for i in range(2):
        last_copy(i).wait_recv()
    mixer_out[...] = summed(0, mixer_part).astype(bf16)
    for c in range(PIECES):
        cols = pl.ds(c * piece, piece)

        def wait_back(k, carry, c=c):
            back_copy(k, c, me, (me + ep_count - k) % ep_count).wait_recv()
            return carry

        lax.fori_loop(1, ep_count, wait_back, 0)
        total = (
            shared_part[parity, level, :, cols].astype(f32)
            + half_in[1, level, :, cols].astype(f32)
            + last_in[1, :, cols].astype(f32)
        )
        for k in range(top):
            total = total + weights_col[k][:, :1] * jnp.dot(
                picks[k], back[:, cols], preferred_element_type=f32
            )
        expert_out[:, cols] = total.astype(bf16)

    for copy in to_far + to_mate + to_pass:
        copy.wait_send()
    for i, part in enumerate((mixer_part, shared_part)):
        half_copy(i, part).wait_send()
        last_copy(i).wait_send()

    def drain(k, carry):
        slot_copy(k, (me + k) % ep_count, me).wait_send()
        for c in range(PIECES):
            back_copy(k, c, (me + k) % ep_count, me).wait_send()
        return carry

    lax.fori_loop(1, ep_count, drain, 0)


def mixture(
    expert_input, mixer_part, gain_expert, expert_choice, route_weights,
    expert_gate, expert_up, expert_down, shared_gate, shared_up, shared_down,
):
    tp_count = lax.axis_size("tp")
    ep_count = lax.axis_size("ep")
    tokens, width = expert_input.shape
    own = tokens // tp_count
    top = expert_choice.shape[1]
    local_experts, _, ff = expert_gate.shape
    shared_ff = shared_gate.shape[1]
    experts_all = local_experts * ep_count
    capacity = -(-(2 * own * top // experts_all) // 16) * 16
    slots = experts_all * capacity
    assert tp_count == 4 and local_experts == 1
    any_spec = pl.BlockSpec(memory_space=pl.ANY)
    vmem_spec = pl.BlockSpec(memory_space=pltpu.VMEM)
    dma = pltpu.SemaphoreType.DMA
    vmem = pltpu.VMEM
    count = 2 + PIECES
    part = mixer_part.reshape(2, 2, own, width).swapaxes(0, 1)
    return pl.pallas_call(
        functools.partial(mixture_kernel, capacity),
        out_shape=(jax.ShapeDtypeStruct((own, width), bf16),) * 2,
        in_specs=[any_spec] * 11,
        out_specs=(vmem_spec,) * 2,
        scratch_shapes=[
            vmem((tokens, width), bf16),
            vmem((tokens, width), bf16),
            vmem((1, width), f32),
            vmem((top, tokens), jnp.int32),
            vmem((top, tokens), f32),
            vmem((tp_count, width, ff), bf16),
            vmem((tp_count, width, ff), bf16),
            vmem((tp_count * ff, width), bf16),
            vmem((width, shared_ff), bf16),
            vmem((width, shared_ff), bf16),
            vmem((shared_ff, width), bf16),
            vmem((own, width), bf16),
            vmem((slots, width), bf16),
            vmem((slots, width), bf16),
            vmem((slots, tp_count * ff), bf16),
            vmem((slots, width), bf16),
            vmem((slots, width), bf16),
            vmem((top, own, slots), bf16),
            vmem((top, own, own), f32),
            vmem((2, 2, own, width), bf16),
            vmem((2, 2, own, width), bf16),
            vmem((tokens, shared_ff), bf16),
            vmem((2, 2, own, width), bf16),
            vmem((2, own, width), bf16),
            vmem((2, own, width), bf16),
            dma((11,)),
            dma((count,)), dma((count,)),
            dma((count,)), dma((count,)),
            dma((count,)), dma((count,)),
            dma((ep_count,)), dma((ep_count,)),
            dma((ep_count, PIECES)), dma((ep_count, PIECES)),
            dma((2,)), dma((2,)),
            dma((2,)), dma((2,)),
        ],
        compiler_params=pltpu.CompilerParams(
            collective_id=0, has_side_effects=True, vmem_limit_bytes=60 * 1024 * 1024
        ),
    )(
        expert_input, part, gain_expert[None, :], expert_choice.T, route_weights.T,
        expert_gate[0], expert_up[0], expert_down[0], shared_gate, shared_up, shared_down,
    )


def local(
    mixer_input,
    expert_input,
    gain_mixer,
    gain_expert,
    query_weight,
    key_weight,
    value_weight,
    sink_logits,
    output_weight,
    expert_choice,
    route_weights,
    expert_gate,
    expert_up,
    expert_down,
    shared_gate,
    shared_up,
    shared_down,
):
    ep_count = lax.axis_size("ep")
    group_rows, model_width = mixer_input.shape
    normed = rms_scale(mixer_input, gain_mixer)
    queries = jnp.dot(normed, query_weight, preferred_element_type=jnp.float32).astype(jnp.bfloat16)
    key_rows = jnp.dot(normed, key_weight, preferred_element_type=jnp.float32).astype(jnp.bfloat16)
    value_rows = jnp.dot(normed, value_weight, preferred_element_type=jnp.float32).astype(
        jnp.bfloat16
    )
    first_position = lax.axis_index("ep") % (ep_count // SEQS) * group_rows
    positions = (first_position + jnp.arange(group_rows, dtype=jnp.int32)).astype(jnp.float32)
    angles = positions[:, None] * frequencies(HEAD_DIM)[None, :]
    rot_queries = rotate(queries.reshape(group_rows, -1, HEAD_DIM), angles)
    rot_keys = rotate(key_rows.reshape(group_rows, -1, HEAD_DIM), angles)
    key_width = key_rows.shape[1]
    tail_start = group_rows - WINDOW
    tail_pair = jnp.concatenate(
        [rot_keys.reshape(group_rows, key_width)[tail_start:], value_rows[tail_start:]], axis=1
    )
    earlier_pair = from_behind(tail_pair, "ep", 1)
    prior_keys = earlier_pair[:, :key_width].reshape(WINDOW, -1, HEAD_DIM)
    prior_values = earlier_pair[:, key_width:].reshape(WINDOW, -1, HEAD_DIM)
    attended = attend(
        rot_queries,
        rot_keys,
        value_rows.reshape(group_rows, -1, HEAD_DIM),
        prior_keys,
        prior_values,
        first_position,
        sink_logits,
    )
    mixer_part = jnp.dot(attended, output_weight, preferred_element_type=jnp.float32).astype(
        jnp.bfloat16
    )
    return mixture(
        expert_input, mixer_part, gain_expert, expert_choice, route_weights,
        expert_gate, expert_up, expert_down, shared_gate, shared_up, shared_down,
    )


def solution(mesh):
    placed = (
        P("ep", None),
        P("ep", None),
        P(),
        P(),
        P(None, "tp"),
        P(None, "tp"),
        P(None, "tp"),
        P("tp"),
        P("tp", None),
        P("ep", None),
        P("ep", None),
        P("ep", None, "tp"),
        P("ep", None, "tp"),
        P("ep", "tp", None),
        P(None, "tp"),
        P(None, "tp"),
        P("tp", None),
    )
    return jax.shard_map(
        local,
        mesh=mesh,
        in_specs=placed,
        out_specs=(P(("ep", "tp"), None), P(("ep", "tp"), None)),
        check_vma=False,
    )
```

```python
import functools

import jax
import jax.numpy as jnp
from jax import lax
from jax.experimental import pallas as pl
from jax.experimental.pallas import tpu as pltpu
from jax.sharding import PartitionSpec as P

HEAD_DIM = 64
WINDOW = 128
SEQS = 1
PIECES = 4

norm_eps = 1e-06
rope_base = 500000.0
bf16 = jnp.bfloat16
f32 = jnp.float32
MESH = pl.DeviceIdType.MESH


def frequencies(head_size):
    half_steps = jnp.arange(head_size // 2, dtype=jnp.float32)
    return rope_base ** (-(2.0 * half_steps) / head_size)


def rows_at(start, count, unit):
    return pl.ds(pl.multiple_of(start, unit), count)


def norm_into(target, source, start, count, gain):
    step = 32

    def body(i, carry):
        widened = source[rows_at(start + i * step, step, step), :].astype(f32)
        scale = lax.rsqrt(jnp.mean(widened * widened, axis=-1, keepdims=True) + norm_eps)
        target[rows_at(i * step, step, step), :] = (widened * scale * gain[...]).astype(bf16)
        return carry

    lax.fori_loop(0, count // step, body, 0)


def silu_times(gate, up):
    return gate / (1.0 + jnp.exp(-gate)) * up


def mixture_kernel(
    capacity,
    x_ref, gain_ref, choice_ref, route_ref,
    wg_ref, wu_ref, wd_ref, sg_ref, su_ref, sd_ref,
    mx_ref, mgain_ref, wq_ref, wk_ref, wv_ref, wo_ref, sink_ref, freq_ref,
    mixer_out, expert_out,
    rows_in, normed, gain, choice, route, wg, wu, wd, sg, su, sd,
    mixer_in, mixer_gain, wq, wk, wv, wo, sink, freq, queries, band, attended,
    own_rows, slots_out, slots_in, hidden, result, back, picks, weights_col,
    mixer_part, shared_part, shared_hidden, half_in, half_out, last_in,
    load_sem, far_send, far_recv, mate_send, mate_recv, pass_send, pass_recv,
    slot_send, slot_recv, back_send, back_recv, half_send, half_recv, last_send, last_recv,
    halo_send, halo_recv,
):
    ep_count = lax.axis_size("ep")
    me = lax.axis_index("ep")
    t = lax.axis_index("tp")
    parity = t % 2
    level = t // 2
    mate = t + 1 - 2 * parity
    far = (t + 2) % 4
    far_mate = (mate + 2) % 4
    tokens, width = rows_in.shape
    own = own_rows.shape[0]
    ff = wd_ref.shape[0]
    slots = slots_out.shape[0]
    piece = width // PIECES

    barrier = pltpu.get_barrier_semaphore()

    def greet(k, carry):
        pl.semaphore_signal(barrier, inc=1, device_id={"ep": (me + k) % ep_count}, device_id_type=MESH)
        return carry

    lax.fori_loop(1, ep_count, greet, 0)
    for other in (mate, far):
        pl.semaphore_signal(barrier, inc=1, device_id={"tp": other}, device_id_type=MESH)

    loads = [
        (gain_ref, gain), (choice_ref, choice), (route_ref, route), (x_ref, rows_in),
        (wg_ref, wg.at[t]), (wu_ref, wu.at[t]), (wd_ref, wd.at[rows_at(t * ff, ff, ff)]),
        (mgain_ref, mixer_gain), (freq_ref, freq), (sink_ref, sink), (mx_ref, mixer_in),
        (wq_ref, wq), (wk_ref, wk), (wv_ref, wv), (sg_ref, sg), (su_ref, su), (sd_ref, sd), (wo_ref, wo),
    ]
    loads = [pltpu.make_async_copy(a, b, load_sem.at[i]) for i, (a, b) in enumerate(loads)]
    for load in loads:
        load.start()

    pl.semaphore_wait(barrier, ep_count + 1)

    def block_views(owner):
        views = [wg.at[owner], wu.at[owner]]
        down = wd.at[rows_at(owner * ff, ff, ff)]
        return views + [down.at[:, pl.ds(c * piece, piece)] for c in range(PIECES)]

    sources = [wg_ref, wu_ref] + [wd_ref.at[:, pl.ds(c * piece, piece)] for c in range(PIECES)]

    def remote(src, dst, send, recv, device):
        return pltpu.make_async_remote_copy(
            src_ref=src, dst_ref=dst, send_sem=send, recv_sem=recv,
            device_id=device, device_id_type=MESH,
        )

    def views_copy(srcs, owner, send, recv, device):
        return [
            remote(a, b, send.at[i], recv.at[i], device)
            for i, (a, b) in enumerate(zip(srcs, block_views(owner)))
        ]

    to_far = views_copy(sources, t, far_send, far_recv, {"tp": far})
    to_mate = views_copy(sources, t, mate_send, mate_recv, {"tp": mate})
    from_far = views_copy(sources, far, far_send, far_recv, {"tp": far})
    from_mate = views_copy(sources, mate, mate_send, mate_recv, {"tp": mate})
    to_pass = views_copy(block_views(far), far, pass_send, pass_recv, {"tp": mate})
    from_pass = views_copy(block_views(far), far_mate, pass_send, pass_recv, {"tp": mate})
    for copy in to_far:
        copy.start()

    for i in (0, 1, 2, 3):
        loads[i].wait()
    norm_into(own_rows, rows_in, t * own, own, gain)
    lanes = rows_at(t * own, own, own)
    top = choice.shape[0]
    chosen = choice[:, lanes]
    row_ids = lax.broadcasted_iota(jnp.int32, (slots // capacity, own), 0)
    named = [row_ids == chosen[k : k + 1, :] for k in range(top)]
    named_any = functools.reduce(jnp.logical_or, named).astype(f32)
    earlier = lax.broadcasted_iota(jnp.int32, (own, own), 0)
    later = lax.broadcasted_iota(jnp.int32, (own, own), 1)
    ranks = jnp.dot(named_any, (earlier < later).astype(f32), preferred_element_type=f32)
    slot_rows = [
        chosen[k : k + 1, :] * capacity
        + jnp.sum(jnp.where(named[k], ranks, 0.0), axis=0, keepdims=True).astype(jnp.int32)
        for k in range(top)
    ]
    slot_ids = lax.broadcasted_iota(jnp.int32, (slots, own), 0)
    spread = functools.reduce(jnp.logical_or, [slot_ids == row for row in slot_rows])
    spread = spread.astype(f32).astype(bf16)
    for c in range(PIECES):
        cols = pl.ds(c * piece, piece)
        slots_out[:, cols] = jnp.dot(spread, own_rows[:, cols], preferred_element_type=f32).astype(bf16)

    def slot_block(ref, owner):
        return ref.at[rows_at(owner * capacity, capacity, capacity)]

    def slot_copy(k, target, origin):
        return remote(
            slot_block(slots_out, target), slot_block(slots_in, origin),
            slot_send.at[k], slot_recv.at[k], {"ep": target},
        )

    def send_slots(k, carry):
        slot_copy(k, (me + k) % ep_count, me).start()
        return carry

    lax.fori_loop(1, ep_count, send_slots, 0)
    for copy in to_mate:
        copy.start()

    own_block = rows_at(me * capacity, capacity, capacity)
    slots_in[own_block, :] = slots_out[own_block, :]
    lane_ids = lax.broadcasted_iota(jnp.int32, (own, slots), 1)
    for k in range(top):
        column = jnp.broadcast_to(slot_rows[k].astype(f32), (own, own)).T[:, :1].astype(jnp.int32)
        picks[k] = (lane_ids == column).astype(f32).astype(bf16)
        weights_col[k] = jnp.broadcast_to(route[k : k + 1, lanes], (own, own)).T

    def half_copy(i, part):
        return remote(
            part.at[1 - parity], half_in.at[i], half_send.at[i], half_recv.at[i], {"tp": mate}
        )

    def last_copy(i):
        return remote(
            half_out.at[i], last_in.at[i], last_send.at[i], last_recv.at[i], {"tp": far}
        )

    def middle(i, part):
        half_copy(i, part).wait_recv()
        half_out[i] = (part[parity, 1 - level].astype(f32) + half_in[i, 1 - level].astype(f32)).astype(bf16)
        last_copy(i).start()

    for i in range(7, 14):
        loads[i].wait()
    norm_into(normed, mixer_in, 0, tokens, mixer_gain)
    pair = 2 * HEAD_DIM
    pairs = wq.shape[1] // pair
    lane = lax.broadcasted_iota(jnp.int32, (1, pair), 1)
    first_half = lane % HEAD_DIM < HEAD_DIM // 2
    lower = lane < HEAD_DIM
    twice = lax.broadcasted_iota(jnp.int32, (HEAD_DIM, pair), 0)
    twice = (lax.broadcasted_iota(jnp.int32, (HEAD_DIM, pair), 1) % HEAD_DIM == twice).astype(f32).astype(bf16)
    first_position = me % (ep_count // SEQS) * tokens
    transposed = (((1,), (1,)), ((), ()))

    def project(i, carry):
        rows = rows_at(i * WINDOW, WINDOW, WINDOW)
        ahead = rows_at((i + 1) * WINDOW, WINDOW, WINDOW)
        source = normed[rows, :]
        position = lax.broadcasted_iota(jnp.int32, (WINDOW, pair), 0) + (first_position + i * WINDOW)
        angles = position.astype(f32) * freq[...]
        cosine = jnp.cos(angles)
        sine = jnp.sin(angles)
        sine = jnp.where(first_half, -sine, sine)

        def turn(heads):
            swapped = jnp.where(
                first_half,
                pltpu.roll(heads, pair - HEAD_DIM // 2, 1),
                pltpu.roll(heads, HEAD_DIM // 2, 1),
            )
            return heads * cosine + swapped * sine

        def rounded(value):
            return value.astype(bf16).astype(f32)

        for j in range(pairs):
            cols = pl.ds(j * pair, pair)
            heads = rounded(jnp.dot(source, wq[:, cols], preferred_element_type=f32))
            queries[rows, cols] = (turn(heads).astype(bf16).astype(f32) * HEAD_DIM ** -0.5).astype(bf16)
        keys = lax.dot_general(source, wk[...], transposed, preferred_element_type=f32).astype(bf16)
        keys = jnp.dot(keys, twice, preferred_element_type=f32)
        band[0, ahead, :] = turn(keys).astype(bf16)
        values = lax.dot_general(source, wv[...], transposed, preferred_element_type=f32).astype(bf16)
        band[1, ahead, :] = jnp.dot(values, twice, preferred_element_type=f32).astype(bf16)
        return carry

    lax.fori_loop(0, tokens // WINDOW, project, 0)

    def halo_copy(target):
        return remote(
            band.at[:, pl.ds(tokens, WINDOW)], band.at[:, pl.ds(0, WINDOW)],
            halo_send, halo_recv, {"ep": target},
        )

    halo_copy((me + 1) % ep_count).start()

    norm_into(normed, rows_in, 0, tokens, gain)
    for i in (14, 15, 16):
        loads[i].wait()
    for r in range(2):
        rows = pl.ds(r * (tokens // 2), tokens // 2)
        gate = jnp.dot(normed[rows, :], sg[...], preferred_element_type=f32)
        up = jnp.dot(normed[rows, :], su[...], preferred_element_type=f32)
        shared_hidden[rows, :] = silu_times(gate, up).astype(bf16)
    for owner in range(4):
        for c in range(PIECES):
            cols = pl.ds(c * piece, piece)
            shared_part[owner % 2, owner // 2, :, cols] = jnp.dot(
                shared_hidden[pl.ds(owner * own, own), :], sd[:, cols], preferred_element_type=f32
            ).astype(bf16)
    half_copy(1, shared_part).start()

    loads[17].wait()
    halo_copy((me + 1) % ep_count).wait_recv()
    count = 2 * pairs
    row = lax.broadcasted_iota(jnp.int32, (WINDOW, 2 * WINDOW), 0)
    key = lax.broadcasted_iota(jnp.int32, (WINDOW, 2 * WINDOW), 1)
    distance = row + WINDOW - key
    in_window = (distance >= 0) & (distance < WINDOW)

    def attend(i, carry):
        rows = rows_at(i * WINDOW, WINDOW, WINDOW)
        reach = rows_at(i * WINDOW, 2 * WINDOW, WINDOW)
        allowed = in_window & (key + (first_position + (i - 1) * WINDOW) >= 0)
        keys = band[0, reach, :]
        values = band[1, reach, :]
        for j in range(pairs):
            cols = pl.ds(j * pair, pair)
            both = queries[rows, cols]
            mixed = []
            for side in range(2):
                head = 2 * j + side
                kept = jnp.where(lower if side == 0 else ~lower, both, jnp.zeros_like(both))
                scores = lax.dot_general(kept, keys, transposed, preferred_element_type=f32)
                scores = jnp.where(allowed, scores, -jnp.inf)
                sunk = sink[:, head : head + 1]
                peak = jnp.maximum(jnp.max(scores, axis=-1, keepdims=True), sunk)
                raised = jnp.exp(scores - peak)
                below = jnp.sum(raised, axis=-1, keepdims=True) + jnp.exp(sunk - peak)
                mixed.append(jnp.dot(raised.astype(bf16), values, preferred_element_type=f32) / below)
            attended[rows, cols] = jnp.where(lower, mixed[0], mixed[1]).astype(bf16)
        return carry

    lax.fori_loop(0, tokens // WINDOW, attend, 0)
    for owner in range(4):
        for c in range(PIECES):
            cols = pl.ds(c * piece, piece)
            mixer_part[owner % 2, owner // 2, :, cols] = jnp.dot(
                attended[pl.ds(owner * own, own), :], wo[:, cols], preferred_element_type=f32
            ).astype(bf16)
    half_copy(0, mixer_part).start()
    middle(0, mixer_part)
    middle(1, shared_part)

    def hidden_block(owner):
        step = 256
        columns = rows_at(owner * ff, ff, ff)

        def body(i, carry):
            rows = rows_at(i * step, step, step)
            gate = jnp.dot(slots_in[rows, :], wg[owner], preferred_element_type=f32)
            up = jnp.dot(slots_in[rows, :], wu[owner], preferred_element_type=f32)
            hidden[rows, columns] = silu_times(gate, up).astype(bf16)
            return carry

        lax.fori_loop(0, slots // step, body, 0)

    from_far[0].wait_recv()
    to_pass[0].start()

    def wait_slots(k, carry):
        slot_copy(k, me, (me + ep_count - k) % ep_count).wait_recv()
        return carry

    lax.fori_loop(1, ep_count, wait_slots, 0)
    for i in (4, 5, 6):
        loads[i].wait()
    hidden_block(t)
    for copy in from_mate:
        copy.wait_recv()
    hidden_block(mate)
    from_far[1].wait_recv()
    to_pass[1].start()
    hidden_block(far)
    for i in (0, 1):
        from_pass[i].wait_recv()
    hidden_block(far_mate)

    def back_copy(k, c, target, origin):
        cols = pl.ds(c * piece, piece)
        return remote(
            slot_block(result, target).at[:, cols], slot_block(back, origin).at[:, cols],
            back_send.at[k, c], back_recv.at[k, c], {"ep": target},
        )

    for c in range(PIECES):
        cols = pl.ds(c * piece, piece)
        from_far[2 + c].wait_recv()
        to_pass[2 + c].start()
        from_pass[2 + c].wait_recv()
        step = 256

        def down(i, carry, cols=cols):
            rows = rows_at(i * step, step, step)
            result[rows, cols] = jnp.dot(
                hidden[rows, :], wd[:, cols], preferred_element_type=f32
            ).astype(bf16)
            return carry

        lax.fori_loop(0, slots // step, down, 0)

        def send_back(k, carry, c=c):
            back_copy(k, c, (me + k) % ep_count, me).start()
            return carry

        lax.fori_loop(1, ep_count, send_back, 0)
        back[own_block, cols] = result[own_block, cols]

    def summed(i, part):
        return part[parity, level].astype(f32) + half_in[i, level].astype(f32) + last_in[i].astype(f32)

    for i in range(2):
        last_copy(i).wait_recv()
    mixer_out[...] = summed(0, mixer_part).astype(bf16)
    for c in range(PIECES):
        cols = pl.ds(c * piece, piece)

        def wait_back(k, carry, c=c):
            back_copy(k, c, me, (me + ep_count - k) % ep_count).wait_recv()
            return carry

        lax.fori_loop(1, ep_count, wait_back, 0)
        total = (
            shared_part[parity, level, :, cols].astype(f32)
            + half_in[1, level, :, cols].astype(f32)
            + last_in[1, :, cols].astype(f32)
        )
        for k in range(top):
            total = total + weights_col[k][:, :1] * jnp.dot(
                picks[k], back[:, cols], preferred_element_type=f32
            )
        expert_out[:, cols] = total.astype(bf16)

    for copy in to_far + to_mate + to_pass:
        copy.wait_send()
    for i, part in enumerate((mixer_part, shared_part)):
        half_copy(i, part).wait_send()
        last_copy(i).wait_send()

    halo_copy((me + 1) % ep_count).wait_send()

    def drain(k, carry):
        slot_copy(k, (me + k) % ep_count, me).wait_send()
        for c in range(PIECES):
            back_copy(k, c, (me + k) % ep_count, me).wait_send()
        return carry

    lax.fori_loop(1, ep_count, drain, 0)


def local(
    mixer_input,
    expert_input,
    gain_mixer,
    gain_expert,
    query_weight,
    key_weight,
    value_weight,
    sink_logits,
    output_weight,
    expert_choice,
    route_weights,
    expert_gate,
    expert_up,
    expert_down,
    shared_gate,
    shared_up,
    shared_down,
):
    tp_count = lax.axis_size("tp")
    ep_count = lax.axis_size("ep")
    tokens, width = expert_input.shape
    own = tokens // tp_count
    top = expert_choice.shape[1]
    local_experts, _, ff = expert_gate.shape
    shared_ff = shared_gate.shape[1]
    experts_all = local_experts * ep_count
    capacity = -(-(2 * own * top // experts_all) // 16) * 16
    slots = experts_all * capacity
    assert tp_count == 4 and local_experts == 1
    heads = query_weight.shape[1] // HEAD_DIM
    assert heads % 2 == 0 and key_weight.shape[1] == HEAD_DIM and own % WINDOW == 0
    hbm_spec = pl.BlockSpec(memory_space=pltpu.HBM)
    vmem_spec = pl.BlockSpec(memory_space=pltpu.VMEM)
    dma = pltpu.SemaphoreType.DMA
    vmem = pltpu.VMEM
    count = 2 + PIECES
    freq = jnp.tile(frequencies(HEAD_DIM), 4)[None, :]
    return pl.pallas_call(
        functools.partial(mixture_kernel, capacity),
        out_shape=(jax.ShapeDtypeStruct((own, width), bf16),) * 2,
        in_specs=[hbm_spec] * 18,
        out_specs=(vmem_spec,) * 2,
        scratch_shapes=[
            vmem((tokens, width), bf16),
            vmem((tokens, width), bf16),
            vmem((1, width), f32),
            vmem((top, tokens), jnp.int32),
            vmem((top, tokens), f32),
            vmem((tp_count, width, ff), bf16),
            vmem((tp_count, width, ff), bf16),
            vmem((tp_count * ff, width), bf16),
            vmem((width, shared_ff), bf16),
            vmem((width, shared_ff), bf16),
            vmem((shared_ff, width), bf16),
            vmem((tokens, width), bf16),
            vmem((1, width), f32),
            vmem(query_weight.shape, bf16),
            vmem((HEAD_DIM, width), bf16),
            vmem((HEAD_DIM, width), bf16),
            vmem(output_weight.shape, bf16),
            vmem((1, heads), f32),
            vmem((1, 2 * HEAD_DIM), f32),
            vmem((tokens, heads * HEAD_DIM), bf16),
            vmem((2, WINDOW + tokens, 2 * HEAD_DIM), bf16),
            vmem((tokens, heads * HEAD_DIM), bf16),
            vmem((own, width), bf16),
            vmem((slots, width), bf16),
            vmem((slots, width), bf16),
            vmem((slots, tp_count * ff), bf16),
            vmem((slots, width), bf16),
            vmem((slots, width), bf16),
            vmem((top, own, slots), bf16),
            vmem((top, own, own), f32),
            vmem((2, 2, own, width), bf16),
            vmem((2, 2, own, width), bf16),
            vmem((tokens, shared_ff), bf16),
            vmem((2, 2, own, width), bf16),
            vmem((2, own, width), bf16),
            vmem((2, own, width), bf16),
            dma((18,)),
            dma((count,)), dma((count,)),
            dma((count,)), dma((count,)),
            dma((count,)), dma((count,)),
            dma((ep_count,)), dma((ep_count,)),
            dma((ep_count, PIECES)), dma((ep_count, PIECES)),
            dma((2,)), dma((2,)),
            dma((2,)), dma((2,)),
            dma, dma,
        ],
        compiler_params=pltpu.CompilerParams(
            collective_id=0, has_side_effects=True, vmem_limit_bytes=56 * 1024 * 1024
        ),
    )(
        expert_input, gain_expert[None, :], expert_choice.T, route_weights.T,
        expert_gate[0], expert_up[0], expert_down[0], shared_gate, shared_up, shared_down,
        mixer_input, gain_mixer[None, :], query_weight, key_weight.T, value_weight.T, output_weight,
        sink_logits[None, :], freq,
    )


def solution(mesh):
    placed = (
        P("ep", None),
        P("ep", None),
        P(),
        P(),
        P(None, "tp"),
        P(None, "tp"),
        P(None, "tp"),
        P("tp"),
        P("tp", None),
        P("ep", None),
        P("ep", None),
        P("ep", None, "tp"),
        P("ep", None, "tp"),
        P("ep", "tp", None),
        P(None, "tp"),
        P(None, "tp"),
        P("tp", None),
    )
    return jax.shard_map(
        local,
        mesh=mesh,
        in_specs=placed,
        out_specs=(P(("ep", "tp"), None), P(("ep", "tp"), None)),
        check_vma=False,
    )
```

```python
import functools

import jax
import jax.numpy as jnp
import numpy as np
from jax import lax
from jax.experimental import pallas as pl
from jax.experimental.pallas import tpu as pltpu
from jax.sharding import PartitionSpec as P

HEAD_DIM = 64
WINDOW = 128
SEQS = 1
PIECES = 4

norm_eps = 1e-06
rope_base = 500000.0
bf16 = jnp.bfloat16
f32 = jnp.float32
MESH = pl.DeviceIdType.MESH


def frequencies(head_size):
    half_steps = np.arange(head_size // 2, dtype=np.float64)
    return np.tile(rope_base ** (-(2.0 * half_steps) / head_size), 4).astype(np.float32)[None, :]


def rows_at(start, count, unit):
    return pl.ds(pl.multiple_of(start, unit), count)


def norm_into(target, source, to, start, count, gain):
    step = 32

    def body(i, carry):
        widened = source[rows_at(start + i * step, step, step), :].astype(f32)
        scale = lax.rsqrt(jnp.mean(widened * widened, axis=-1, keepdims=True) + norm_eps)
        target[rows_at(to + i * step, step, step), :] = (widened * scale * gain[...]).astype(bf16)
        return carry

    lax.fori_loop(0, count // step, body, 0)


def silu_times(gate, up):
    return gate / (1.0 + jnp.exp(-gate)) * up


def mixture_kernel(
    capacity,
    x_ref, gain_ref, choice_ref, route_ref,
    wg_ref, wu_ref, wd_ref, sg_ref, su_ref, sd_ref,
    mx_ref, mgain_ref, wq_ref, wk_ref, wv_ref, wo_ref, sink_ref, freq_ref,
    mixer_out, expert_out,
    rows_in, normed, gain, choice, route, wg, wu, wd, sg, su, sd,
    mixer_in, mixer_gain, wq, wk, wv, wo, sink, sunk, freq, cosines, sines, queries, band, attended,
    own_rows, slots_out, slots_in, hidden, result, back, picks, weights_col,
    mirror_choice, mirror_route, mirror_picks, mirror_weights, dense_out, dense_in, expert_sum,
    mixer_part, shared_part, shared_hidden, half_in, half_out, last_in,
    load_sem, far_send, far_recv, mate_send, mate_recv, pass_send, pass_recv,
    slot_send, slot_recv, back_send, back_recv, half_send, half_recv, last_send, last_recv,
    halo_send, halo_recv, mirror_send, mirror_recv, dense_send, dense_recv,
):
    ep_count = lax.axis_size("ep")
    me = lax.axis_index("ep")
    t = lax.axis_index("tp")
    parity = t % 2
    level = t // 2
    mate = t + 1 - 2 * parity
    far = (t + 2) % 4
    far_mate = (mate + 2) % 4
    tokens, width = rows_in.shape
    own = own_rows.shape[0]
    ff = wd_ref.shape[0]
    slots = slots_out.shape[0]
    piece = width // PIECES

    barrier = pltpu.get_barrier_semaphore()

    def greet(k, carry):
        pl.semaphore_signal(barrier, inc=1, device_id={"ep": (me + k) % ep_count}, device_id_type=MESH)
        return carry

    lax.fori_loop(1, ep_count, greet, 0)
    for other in (mate, far):
        pl.semaphore_signal(barrier, inc=1, device_id={"tp": other}, device_id_type=MESH)

    loads = [
        (gain_ref, gain), (choice_ref, choice), (route_ref, route), (x_ref, rows_in),
        (mgain_ref, mixer_gain), (freq_ref, freq), (mx_ref, mixer_in), (wk_ref, wk), (wv_ref, wv),
        (wq_ref, wq), (sink_ref, sink), (sg_ref, sg), (su_ref, su), (sd_ref, sd), (wo_ref, wo),
        (wg_ref, wg.at[t]), (wu_ref, wu.at[t]), (wd_ref, wd.at[rows_at(t * ff, ff, ff)]),
    ]
    loads = [pltpu.make_async_copy(a, b, load_sem.at[i]) for i, (a, b) in enumerate(loads)]
    for load in loads:
        load.start()

    pl.semaphore_wait(barrier, ep_count + 1)

    def block_views(owner):
        views = [wg.at[owner], wu.at[owner]]
        down = wd.at[rows_at(owner * ff, ff, ff)]
        return views + [down.at[:, pl.ds(c * piece, piece)] for c in range(PIECES)]

    sources = [wg_ref, wu_ref] + [wd_ref.at[:, pl.ds(c * piece, piece)] for c in range(PIECES)]

    def remote(src, dst, send, recv, device):
        return pltpu.make_async_remote_copy(
            src_ref=src, dst_ref=dst, send_sem=send, recv_sem=recv,
            device_id=device, device_id_type=MESH,
        )

    def views_copy(srcs, owner, send, recv, device):
        return [
            remote(a, b, send.at[i], recv.at[i], device)
            for i, (a, b) in enumerate(zip(srcs, block_views(owner)))
        ]

    to_far = views_copy(sources, t, far_send, far_recv, {"tp": far})
    to_mate = views_copy(sources, t, mate_send, mate_recv, {"tp": mate})
    from_far = views_copy(sources, far, far_send, far_recv, {"tp": far})
    from_mate = views_copy(sources, mate, mate_send, mate_recv, {"tp": mate})
    to_pass = views_copy(block_views(far), far, pass_send, pass_recv, {"tp": mate})
    from_pass = views_copy(block_views(far), far_mate, pass_send, pass_recv, {"tp": mate})
    for copy in to_far:
        copy.start()

    for i in (0, 1, 2, 3):
        loads[i].wait()
    norm_into(own_rows, rows_in, 0, t * own, own, gain)
    lanes = rows_at(t * own, own, own)
    top = choice.shape[0]
    row_ids = lax.broadcasted_iota(jnp.int32, (slots // capacity, own), 0)
    earlier = lax.broadcasted_iota(jnp.int32, (own, own), 0)
    later = lax.broadcasted_iota(jnp.int32, (own, own), 1)
    before = (earlier < later).astype(f32)

    def slots_of(choices):
        chosen = choices[:, lanes]
        named = [row_ids == chosen[k : k + 1, :] for k in range(top)]
        named_any = functools.reduce(jnp.logical_or, named).astype(f32)
        ranks = jnp.dot(named_any, before, preferred_element_type=f32)
        return [
            chosen[k : k + 1, :] * capacity
            + jnp.sum(jnp.where(named[k], ranks, 0.0), axis=0, keepdims=True).astype(jnp.int32)
            for k in range(top)
        ]

    def column_of(row):
        return jnp.broadcast_to(row.astype(f32), (own, own)).T

    slot_rows = slots_of(choice)
    slot_ids = lax.broadcasted_iota(jnp.int32, (slots, own), 0)
    spread = functools.reduce(jnp.logical_or, [slot_ids == row for row in slot_rows])
    spread = spread.astype(f32).astype(bf16)
    for c in range(PIECES):
        cols = pl.ds(c * piece, piece)
        slots_out[:, cols] = jnp.dot(spread, own_rows[:, cols], preferred_element_type=f32).astype(bf16)

    def slot_block(ref, owner):
        return ref.at[rows_at(owner * capacity, capacity, capacity)]

    def slot_copy(k, target, origin):
        return remote(
            slot_block(slots_out, target), slot_block(slots_in, origin),
            slot_send.at[k], slot_recv.at[k], {"ep": target},
        )

    def send_slots(k, carry):
        slot_copy(k, (me + k) % ep_count, me).start()
        return carry

    ahead_of_halo = ep_count // 2
    lax.fori_loop(ep_count // 4, ahead_of_halo, send_slots, 0)

    for i in range(4, 9):
        loads[i].wait()
    pair = 2 * HEAD_DIM
    lane = lax.broadcasted_iota(jnp.int32, (1, pair), 1)
    first_half = lane % HEAD_DIM < HEAD_DIM // 2
    lower = lane < HEAD_DIM
    twice = lax.broadcasted_iota(jnp.int32, (HEAD_DIM, pair), 0)
    twice = (lax.broadcasted_iota(jnp.int32, (HEAD_DIM, pair), 1) % HEAD_DIM == twice).astype(f32).astype(bf16)
    first_position = me % (ep_count // SEQS) * tokens
    transposed = (((1,), (1,)), ((), ()))

    def turn(heads, rows):
        swapped = jnp.where(
            first_half,
            pltpu.roll(heads, pair - HEAD_DIM // 2, 1),
            pltpu.roll(heads, HEAD_DIM // 2, 1),
        )
        return heads * cosines[rows, :] + swapped * sines[rows, :]

    def project_keys(i, carry):
        rows = rows_at(i * WINDOW, WINDOW, WINDOW)
        after = rows_at((i + 1) * WINDOW, WINDOW, WINDOW)
        norm_into(normed, mixer_in, i * WINDOW, i * WINDOW, WINDOW, mixer_gain)
        position = lax.broadcasted_iota(jnp.int32, (WINDOW, pair), 0) + (first_position + i * WINDOW)
        angles = position.astype(f32) * freq[...]
        sine = jnp.sin(angles)
        cosines[rows, :] = jnp.cos(angles)
        sines[rows, :] = jnp.where(first_half, -sine, sine)
        source = normed[rows, :]
        keys = lax.dot_general(source, wk[...], transposed, preferred_element_type=f32).astype(bf16)
        keys = jnp.dot(keys, twice, preferred_element_type=f32)
        band[0, after, :] = turn(keys, rows).astype(bf16)
        values = lax.dot_general(source, wv[...], transposed, preferred_element_type=f32).astype(bf16)
        band[1, after, :] = jnp.dot(values, twice, preferred_element_type=f32).astype(bf16)
        return carry

    def halo_copy(target):
        return remote(
            band.at[:, pl.ds(tokens, WINDOW)], band.at[:, pl.ds(0, WINDOW)],
            halo_send, halo_recv, {"ep": target},
        )

    last_block = tokens // WINDOW - 1
    project_keys(last_block, 0)
    halo_copy((me + 1) % ep_count).start()
    lax.fori_loop(ahead_of_halo, ep_count, send_slots, 0)
    lax.fori_loop(1, ep_count // 4, send_slots, 0)
    for copy in to_mate:
        copy.start()

    quarter_size = ep_count // 4
    quarter = me // quarter_size
    seat = me % quarter_size
    high = quarter // 2
    middle_one = (quarter + high) % 2
    mirror = (3 - quarter) * quarter_size + seat
    side_rows = 2 * quarter_size * capacity
    mirrored = [
        remote(a, b, mirror_send.at[i], mirror_recv.at[i], {"ep": mirror})
        for i, (a, b) in enumerate(((choice, mirror_choice), (route, mirror_route)))
    ]
    for copy in mirrored:
        copy.start()
    own_block = rows_at(me * capacity, capacity, capacity)
    slots_in[own_block, :] = slots_out[own_block, :]
    lane_ids = lax.broadcasted_iota(jnp.int32, (own, slots), 1)
    for k in range(top):
        picks[k] = (lane_ids == column_of(slot_rows[k])[:, :1].astype(jnp.int32)).astype(f32).astype(bf16)
        weights_col[k] = column_of(route[k : k + 1, lanes])

    @pl.when(middle_one == 1)
    def _():
        back[rows_at((1 - high) * side_rows, side_rows, capacity), :] = jnp.zeros((side_rows, width), bf16)

    @pl.when(middle_one == 0)
    def _():
        dense_in[...] = jnp.zeros((own, width), bf16)

    def half_copy(i, part):
        return remote(
            part.at[1 - parity], half_in.at[i], half_send.at[i], half_recv.at[i], {"tp": mate}
        )

    def last_copy(i):
        return remote(
            half_out.at[i], last_in.at[i], last_send.at[i], last_recv.at[i], {"tp": far}
        )

    def middle(i, part):
        half_copy(i, part).wait_recv()
        half_out[i] = (part[parity, 1 - level].astype(f32) + half_in[i, 1 - level].astype(f32)).astype(bf16)
        last_copy(i).start()

    lax.fori_loop(0, last_block, project_keys, 0)
    loads[9].wait()
    pairs = wq.shape[1] // pair

    def project(i, carry):
        rows = rows_at(i * WINDOW, WINDOW, WINDOW)
        for j in range(pairs):
            cols = pl.ds(j * pair, pair)
            heads = jnp.dot(normed[rows, :], wq[:, cols], preferred_element_type=f32)
            turned_heads = turn(heads.astype(bf16).astype(f32), rows).astype(bf16)
            queries[rows, cols] = (turned_heads.astype(f32) * HEAD_DIM ** -0.5).astype(bf16)
        return carry

    lax.fori_loop(0, tokens // WINDOW, project, 0)

    norm_into(normed, rows_in, 0, 0, tokens, gain)
    for i in (11, 12, 13):
        loads[i].wait()
    for r in range(2):
        rows = pl.ds(r * (tokens // 2), tokens // 2)
        gate = jnp.dot(normed[rows, :], sg[...], preferred_element_type=f32)
        up = jnp.dot(normed[rows, :], su[...], preferred_element_type=f32)
        shared_hidden[rows, :] = silu_times(gate, up).astype(bf16)
    for owner in range(4):
        for c in range(PIECES):
            cols = pl.ds(c * piece, piece)
            shared_part[owner % 2, owner // 2, :, cols] = jnp.dot(
                shared_hidden[pl.ds(owner * own, own), :], sd[:, cols], preferred_element_type=f32
            ).astype(bf16)
    half_copy(1, shared_part).start()

    for i in (10, 14):
        loads[i].wait()
    halo_copy((me + 1) % ep_count).wait_recv()
    count = 2 * pairs
    row = lax.broadcasted_iota(jnp.int32, (WINDOW, 2 * WINDOW), 0)
    key = lax.broadcasted_iota(jnp.int32, (WINDOW, 2 * WINDOW), 1)
    distance = row + WINDOW - key
    in_window = (distance >= 0) & (distance < WINDOW)

    for head in range(count):
        sunk[pl.ds(head * WINDOW, WINDOW), :] = jnp.broadcast_to(sink[:, head : head + 1], (WINDOW, pair))

    def attend(i, carry):
        rows = rows_at(i * WINDOW, WINDOW, WINDOW)
        reach = rows_at(i * WINDOW, 2 * WINDOW, WINDOW)
        allowed = in_window & (key + (first_position + (i - 1) * WINDOW) >= 0)
        both = [queries[rows, pl.ds(j * pair, pair)] for j in range(pairs)]
        none = jnp.zeros((WINDOW, pair), bf16)
        kept = jnp.concatenate(
            [jnp.where(side, heads, none) for heads in both for side in (lower, ~lower)], axis=0
        )
        scores = lax.dot_general(kept, band[0, reach, :], transposed, preferred_element_type=f32)
        scores = jnp.where(allowed[None], scores.reshape(count, WINDOW, 2 * WINDOW), -jnp.inf)
        scores = scores.reshape(count * WINDOW, 2 * WINDOW)
        sinks = sunk[:, :1]
        peak = jnp.maximum(jnp.max(scores, axis=-1, keepdims=True), sinks)
        raised = jnp.exp(scores - peak).astype(bf16)
        values = jnp.concatenate([band[1, reach, :], jnp.ones((2 * WINDOW, pair), bf16)], axis=1)
        mixed = jnp.dot(raised, values, preferred_element_type=f32)
        mixed = (mixed[:, :pair] / (mixed[:, pair:] + jnp.exp(sinks - peak))).reshape(count, WINDOW, pair)
        for j in range(pairs):
            attended[rows, pl.ds(j * pair, pair)] = jnp.where(
                lower, mixed[2 * j], mixed[2 * j + 1]
            ).astype(bf16)
        return carry

    lax.fori_loop(0, tokens // WINDOW, attend, 0)
    for owner in range(4):
        for c in range(PIECES):
            cols = pl.ds(c * piece, piece)
            mixer_part[owner % 2, owner // 2, :, cols] = jnp.dot(
                attended[pl.ds(owner * own, own), :], wo[:, cols], preferred_element_type=f32
            ).astype(bf16)
    half_copy(0, mixer_part).start()
    middle(0, mixer_part)
    middle(1, shared_part)

    def hidden_block(owner, side):
        rows = rows_at(side * side_rows, side_rows, capacity)
        gate = jnp.dot(slots_in[rows, :], wg[owner], preferred_element_type=f32)
        up = jnp.dot(slots_in[rows, :], wu[owner], preferred_element_type=f32)
        hidden[rows, rows_at(owner * ff, ff, ff)] = silu_times(gate, up).astype(bf16)

    from_far[0].wait_recv()
    to_pass[0].start()

    def wait_slots(side):
        def wait_one(k, carry):
            source = (me + ep_count - k) % ep_count

            @pl.when(source // (2 * quarter_size) == side)
            def _():
                slot_copy(k, me, source).wait_recv()

            return carry

        lax.fori_loop(1, ep_count, wait_one, 0)

    wait_slots(high)
    for i in (15, 16, 17):
        loads[i].wait()
    hidden_block(t, high)
    for copy in from_mate:
        copy.wait_recv()
    hidden_block(mate, high)
    from_far[1].wait_recv()
    to_pass[1].start()
    hidden_block(far, high)
    wait_slots(1 - high)
    hidden_block(t, 1 - high)
    hidden_block(mate, 1 - high)
    hidden_block(far, 1 - high)
    for i in (0, 1):
        from_pass[i].wait_recv()
    hidden_block(far_mate, high)
    hidden_block(far_mate, 1 - high)

    def is_low_middle(q):
        return (q % 2) * (1 - q // 2)

    def is_high_middle(q):
        return (q // 2) * (1 - q % 2)

    def turned(source, target):
        return is_low_middle(target) * (source // 2) + is_high_middle(target) * (1 - source // 2)

    def landing(source, source_seat, target):
        stop = turned(source, target)
        straight = source * quarter_size + source_seat
        return (1 - stop) * straight + stop * (ep_count + (source % 2) * quarter_size + source_seat)

    def back_copy(k, c, owner, target, block):
        cols = pl.ds(c * piece, piece)
        return remote(
            slot_block(result, owner).at[:, cols], slot_block(back, block).at[:, cols],
            back_send.at[k, c], back_recv.at[block, c], {"ep": target},
        )

    def each_back(c, remote_do, local_do):
        for n, q in enumerate((1, 0, 2, 3)):
            target = high * q + (1 - high) * (3 - q)
            stop = turned(quarter, target)
            via = target + stop * (2 * high - 1)

            def step(j, carry, n=n, target=target, via=via):
                to_seat = (seat + j) % quarter_size
                owner = target * quarter_size + to_seat
                device = via * quarter_size + to_seat
                block = landing(quarter, seat, target)

                @pl.when(device != me)
                def _():
                    remote_do(back_copy(n * quarter_size + j, c, owner, device, block))

                if local_do is not None:
                    @pl.when(device == me)
                    def _():
                        local_do(owner, block)

                return carry

            lax.fori_loop(0, quarter_size, step, 0)

    def wait_block(c, block):
        back_copy(0, c, me, me, block).wait_recv()

    def dense_copy(c):
        cols = pl.ds(c * piece, piece)
        return remote(
            dense_out.at[:, cols], dense_in.at[:, cols], dense_send.at[c], dense_recv.at[c], {"ep": mirror}
        )

    def relay(c):
        cols = pl.ds(c * piece, piece)

        @pl.when(middle_one == 1)
        def _():
            def wait_relayed(n, carry):
                @pl.when(n != (quarter % 2) * quarter_size + seat)
                def _():
                    wait_block(c, ep_count + n)

                return carry

            lax.fori_loop(0, 2 * quarter_size, wait_relayed, 0)
            total = 0.0
            for k in range(top):
                total = total + mirror_weights[k][:, :1] * jnp.dot(
                    mirror_picks[k], back[pl.ds(slots, side_rows), cols], preferred_element_type=f32
                )
            dense_out[:, cols] = total.astype(bf16)
            dense_copy(c).start()

    for copy in mirrored:
        copy.wait_recv()
    near_ids = lax.broadcasted_iota(jnp.int32, (own, side_rows), 1) + high * side_rows
    for k, row in enumerate(slots_of(mirror_choice)):
        mirror_picks[k] = (near_ids == column_of(row)[:, :1].astype(jnp.int32)).astype(f32).astype(bf16)
        mirror_weights[k] = column_of(mirror_route[k : k + 1, lanes])

    for c in range(PIECES):
        cols = pl.ds(c * piece, piece)
        from_far[2 + c].wait_recv()
        to_pass[2 + c].start()
        from_pass[2 + c].wait_recv()
        step = 256

        def down(i, carry, cols=cols):
            rows = rows_at(i * step, step, step)
            result[rows, cols] = jnp.dot(
                hidden[rows, :], wd[:, cols], preferred_element_type=f32
            ).astype(bf16)
            return carry

        lax.fori_loop(0, slots // step, down, 0)

        def keep(owner, block, cols=cols):
            back[rows_at(block * capacity, capacity, capacity), cols] = result[
                rows_at(owner * capacity, capacity, capacity), cols
            ]

        each_back(c, lambda copy: copy.start(), keep)
        if c > 0:
            relay(c - 1)
    relay(PIECES - 1)

    def summed(i, part):
        return part[parity, level].astype(f32) + half_in[i, level].astype(f32) + last_in[i].astype(f32)

    for c in range(PIECES):
        cols = pl.ds(c * piece, piece)

        def wait_back(k, carry, c=c):
            source = (me + ep_count - k) % ep_count

            @pl.when(turned(source // quarter_size, quarter) == 0)
            def _():
                wait_block(c, source)

            return carry

        lax.fori_loop(1, ep_count, wait_back, 0)

        @pl.when(middle_one == 1)
        def _(c=c):
            dense_copy(c).wait_recv()

        total = (
            shared_part[parity, level, :, cols].astype(f32)
            + half_in[1, level, :, cols].astype(f32)
            + dense_in[:, cols].astype(f32)
        )
        for k in range(top):
            total = total + weights_col[k][:, :1] * jnp.dot(
                picks[k], back[pl.ds(0, slots), cols], preferred_element_type=f32
            )
        expert_sum[:, cols] = total
    last_copy(0).wait_recv()
    mixer_out[...] = summed(0, mixer_part)
    last_copy(1).wait_recv()
    expert_out[...] = expert_sum[...] + last_in[1].astype(f32)

    for copy in to_far + to_mate + to_pass:
        copy.wait_send()
    for i, part in enumerate((mixer_part, shared_part)):
        half_copy(i, part).wait_send()
        last_copy(i).wait_send()

    halo_copy((me + 1) % ep_count).wait_send()

    def drain(k, carry):
        slot_copy(k, (me + k) % ep_count, me).wait_send()
        return carry

    lax.fori_loop(1, ep_count, drain, 0)
    for copy in mirrored:
        copy.wait_send()
    for c in range(PIECES):
        each_back(c, lambda copy: copy.wait_send(), None)

        @pl.when(middle_one == 1)
        def _(c=c):
            dense_copy(c).wait_send()


def local(
    mixer_input,
    expert_input,
    gain_mixer,
    gain_expert,
    query_weight,
    key_weight,
    value_weight,
    sink_logits,
    output_weight,
    expert_choice,
    route_weights,
    expert_gate,
    expert_up,
    expert_down,
    shared_gate,
    shared_up,
    shared_down,
):
    tp_count = lax.axis_size("tp")
    ep_count = lax.axis_size("ep")
    tokens, width = expert_input.shape
    own = tokens // tp_count
    top = expert_choice.shape[1]
    local_experts, _, ff = expert_gate.shape
    shared_ff = shared_gate.shape[1]
    experts_all = local_experts * ep_count
    capacity = -(-(2 * own * top // experts_all) // 16) * 16
    slots = experts_all * capacity
    side_rows = slots // 2
    assert tp_count == 4 and local_experts == 1 and ep_count % 4 == 0
    heads = query_weight.shape[1] // HEAD_DIM
    assert heads % 2 == 0 and key_weight.shape[1] == HEAD_DIM and own % WINDOW == 0
    hbm_spec = pl.BlockSpec(memory_space=pltpu.HBM)
    vmem_spec = pl.BlockSpec(memory_space=pltpu.VMEM)
    dma = pltpu.SemaphoreType.DMA
    vmem = pltpu.VMEM
    count = 2 + PIECES
    sums = pl.pallas_call(
        functools.partial(mixture_kernel, capacity),
        out_shape=(jax.ShapeDtypeStruct((own, width), f32),) * 2,
        in_specs=[hbm_spec] * 18,
        out_specs=(vmem_spec,) * 2,
        scratch_shapes=[
            vmem((tokens, width), bf16),
            vmem((tokens, width), bf16),
            vmem((1, width), f32),
            vmem((top, tokens), jnp.int32),
            vmem((top, tokens), f32),
            vmem((tp_count, width, ff), bf16),
            vmem((tp_count, width, ff), bf16),
            vmem((tp_count * ff, width), bf16),
            vmem((width, shared_ff), bf16),
            vmem((width, shared_ff), bf16),
            vmem((shared_ff, width), bf16),
            vmem((tokens, width), bf16),
            vmem((1, width), f32),
            vmem(query_weight.shape, bf16),
            vmem((HEAD_DIM, width), bf16),
            vmem((HEAD_DIM, width), bf16),
            vmem(output_weight.shape, bf16),
            vmem((1, heads), f32),
            vmem((heads * WINDOW, 2 * HEAD_DIM), f32),
            vmem((1, 2 * HEAD_DIM), f32),
            vmem((tokens, 2 * HEAD_DIM), f32),
            vmem((tokens, 2 * HEAD_DIM), f32),
            vmem((tokens, heads * HEAD_DIM), bf16),
            vmem((2, WINDOW + tokens, 2 * HEAD_DIM), bf16),
            vmem((tokens, heads * HEAD_DIM), bf16),
            vmem((own, width), bf16),
            vmem((slots, width), bf16),
            vmem((slots, width), bf16),
            vmem((slots, tp_count * ff), bf16),
            vmem((slots, width), bf16),
            vmem((slots + side_rows, width), bf16),
            vmem((top, own, slots), bf16),
            vmem((top, own, own), f32),
            vmem((top, tokens), jnp.int32),
            vmem((top, tokens), f32),
            vmem((top, own, side_rows), bf16),
            vmem((top, own, own), f32),
            vmem((own, width), bf16),
            vmem((own, width), bf16),
            vmem((own, width), f32),
            vmem((2, 2, own, width), bf16),
            vmem((2, 2, own, width), bf16),
            vmem((tokens, shared_ff), bf16),
            vmem((2, 2, own, width), bf16),
            vmem((2, own, width), bf16),
            vmem((2, own, width), bf16),
            dma((18,)),
            dma((count,)), dma((count,)),
            dma((count,)), dma((count,)),
            dma((count,)), dma((count,)),
            dma((ep_count,)), dma((ep_count,)),
            dma((ep_count, PIECES)), dma((ep_count + ep_count // 2, PIECES)),
            dma((2,)), dma((2,)),
            dma((2,)), dma((2,)),
            dma, dma,
            dma((2,)), dma((2,)),
            dma((PIECES,)), dma((PIECES,)),
        ],
        compiler_params=pltpu.CompilerParams(
            collective_id=0, has_side_effects=True, vmem_limit_bytes=62 * 1024 * 1024
        ),
    )(
        expert_input, gain_expert[None, :], expert_choice.T, route_weights.T,
        expert_gate[0], expert_up[0], expert_down[0], shared_gate, shared_up, shared_down,
        mixer_input, gain_mixer[None, :], query_weight, key_weight.T, value_weight.T, output_weight,
        sink_logits[None, :], frequencies(HEAD_DIM),
    )
    return tuple(value.astype(bf16) for value in sums)


def solution(mesh):
    placed = (
        P("ep", None),
        P("ep", None),
        P(),
        P(),
        P(None, "tp"),
        P(None, "tp"),
        P(None, "tp"),
        P("tp"),
        P("tp", None),
        P("ep", None),
        P("ep", None),
        P("ep", None, "tp"),
        P("ep", None, "tp"),
        P("ep", "tp", None),
        P(None, "tp"),
        P(None, "tp"),
        P("tp", None),
    )
    return jax.shard_map(
        local,
        mesh=mesh,
        in_specs=placed,
        out_specs=(P(("ep", "tp"), None), P(("ep", "tp"), None)),
        check_vma=False,
    )
```

```python
import functools

import jax
import jax.numpy as jnp
import numpy as np
from jax import lax
from jax.experimental import pallas as pl
from jax.experimental.pallas import tpu as pltpu
from jax.sharding import PartitionSpec as P

HEAD_DIM = 64
WINDOW = 128
SEQS = 1
PIECES = 8
BLOCKS = 4
LAG = 2
EARLY = 6

norm_eps = 1e-06
rope_base = 500000.0
bf16 = jnp.bfloat16
f32 = jnp.float32
MESH = pl.DeviceIdType.MESH


def frequencies(head_size):
    half_steps = np.arange(head_size // 2, dtype=np.float64)
    return np.tile(rope_base ** (-(2.0 * half_steps) / head_size), 4).astype(np.float32)[None, :]


def rows_at(start, count, unit):
    return pl.ds(pl.multiple_of(start, unit), count)


def norm_into(target, source, to, start, count, gain):
    step = 32

    def body(i, carry):
        widened = source[rows_at(start + i * step, step, step), :].astype(f32)
        scale = lax.rsqrt(jnp.mean(widened * widened, axis=-1, keepdims=True) + norm_eps)
        target[rows_at(to + i * step, step, step), :] = (widened * scale * gain[...]).astype(bf16)
        return carry

    lax.fori_loop(0, count // step, body, 0)


def silu_times(gate, up):
    return gate / (1.0 + jnp.exp(-gate)) * up


def mixture_kernel(
    capacity,
    x_ref, gain_ref, choice_ref, route_ref,
    wg_ref, wu_ref, wd_ref, sg_ref, su_ref, sd_ref,
    mx_ref, mgain_ref, wq_ref, wk_ref, wv_ref, wo_ref, sink_ref, freq_ref,
    mixer_out, expert_out,
    rows_in, normed, gain, choice, route, wgu, wd, sg, su, sd,
    mixer_in, mixer_gain, wq, wk, wv, wo, sink, sunk, freq, cosines, sines, queries, band, attended,
    own_rows, slots_out, slots_in, hidden, result, back, picks, weights_col,
    mirror_choice, mirror_route, mirror_picks, mirror_weights, dense_out, dense_in, expert_sum,
    mixer_part, shared_hidden, shared_all, half_in, half_out, last_in, mirror_rows, mirror_slots,
    load_sem, far_send, far_recv, mate_send, mate_recv, pass_send, pass_recv,
    slot_send, slot_recv, back_send, back_recv, half_send, half_recv, last_send, last_recv,
    halo_send, halo_recv, mirror_send, mirror_recv, dense_send, dense_recv,
    dealt_send, row_send, row_recv, hid_send, hid_recv, sd_send, sd_recv,
):
    ep_count = lax.axis_size("ep")
    me = lax.axis_index("ep")
    t = lax.axis_index("tp")
    parity = t % 2
    level = t // 2
    mate = t + 1 - 2 * parity
    far = (t + 2) % 4
    far_mate = (mate + 2) % 4
    tokens, width = rows_in.shape
    own = own_rows.shape[0]
    quarter_size = ep_count // 4
    quarter = me // quarter_size
    seat = me % quarter_size
    high = quarter // 2
    middle_one = (quarter + high) % 2
    mirror = (3 - quarter) * quarter_size + seat
    side_rows = 2 * quarter_size * capacity
    ff = wd_ref.shape[0]
    shared_ff = sd_ref.shape[0]
    block = width // BLOCKS
    slots = slots_out.shape[0]
    piece = width // PIECES

    barrier = pltpu.get_barrier_semaphore()

    def greet(k, carry):
        pl.semaphore_signal(barrier, inc=1, device_id={"ep": (me + k) % ep_count}, device_id_type=MESH)
        return carry

    lax.fori_loop(1, ep_count, greet, 0)
    for other in (mate, far, far_mate):
        pl.semaphore_signal(barrier, inc=1, device_id={"tp": other}, device_id_type=MESH)

    part = ff // 2
    halves = [pl.ds(h * part, part) for h in range(2)]
    gate_up_sources = [ref.at[:, half] for half in halves for ref in (wg_ref, wu_ref)]
    sources = gate_up_sources + [wd_ref.at[:, pl.ds(c * piece, piece)] for c in range(PIECES)]

    def gate_up_views(owner):
        return [wgu.at[owner, i] for i in range(4)]

    wide = width // 2

    def sd_view(owner, half):
        return sd.at[half, rows_at(owner * shared_ff, shared_ff, shared_ff)]

    def block_views(owner):
        return gate_up_views(owner) + [wd.at[c, rows_at(owner * ff, ff, ff)] for c in range(PIECES)]

    loads = [
        (gain_ref, gain), (choice_ref, choice), (route_ref, route), (x_ref, rows_in),
        (mgain_ref, mixer_gain), (freq_ref, freq), (mx_ref, mixer_in), (wk_ref, wk), (wv_ref, wv),
        (wq_ref, wq), (sink_ref, sink), (sg_ref, sg), (su_ref, su), (wo_ref, wo),
    ]
    loads += [(sd_ref.at[:, pl.ds(h * wide, wide)], sd_view(t, h)) for h in range(2)]
    loads += list(zip(sources, block_views(t)))
    loads = [pltpu.make_async_copy(a, b, load_sem.at[i]) for i, (a, b) in enumerate(loads)]
    for load in loads:
        load.start()

    pl.semaphore_wait(barrier, ep_count + 2)

    def remote(src, dst, send, recv, device):
        return pltpu.make_async_remote_copy(
            src_ref=src, dst_ref=dst, send_sem=send, recv_sem=recv,
            device_id=device, device_id_type=MESH,
        )

    def views_copy(srcs, owner, send, recv, device):
        return [
            remote(a, b, send.at[i], recv.at[i], device)
            for i, (a, b) in enumerate(zip(srcs, block_views(owner)))
        ]

    to_far = views_copy(sources, t, far_send, far_recv, {"tp": far})
    to_mate = views_copy(sources, t, mate_send, mate_recv, {"tp": mate})
    from_far = views_copy(sources, far, far_send, far_recv, {"tp": far})
    from_mate = views_copy(sources, mate, mate_send, mate_recv, {"tp": mate})
    to_pass = views_copy(block_views(far), far, pass_send, pass_recv, {"tp": mate})
    from_pass = views_copy(block_views(far), far_mate, pass_send, pass_recv, {"tp": mate})
    side_bit = me % 2
    beside = me + 1 - 2 * side_bit
    sd_to_far = remote(
        sd_ref.at[:, rows_at(side_bit * wide, wide, wide)], sd_view(t, side_bit),
        sd_send.at[0], sd_recv.at[0], {"tp": far},
    )
    sd_from_far = remote(sd_view(far, side_bit), sd_view(far, side_bit), sd_send.at[0], sd_recv.at[0], {"tp": far})
    sd_to_beside = remote(sd_view(far, side_bit), sd_view(far, side_bit), sd_send.at[1], sd_recv.at[1], {"ep": beside})
    sd_from_beside = remote(sd_view(far, 1 - side_bit), sd_view(far, 1 - side_bit), sd_send.at[1], sd_recv.at[1], {"ep": beside})
    sd_to_mate, sd_from_mate = (
        [
            remote(sd_ref.at[:, pl.ds(h * wide, wide)], sd_view(owner, h), sd_send.at[4 + h], sd_recv.at[4 + h], {"tp": mate})
            for h in range(2)
        ]
        for owner in (t, mate)
    )
    sd_passed = [
        (
            remote(sd_view(far, half), sd_view(far, half), sd_send.at[2 + i], sd_recv.at[2 + i], {"tp": mate}),
            remote(sd_view(far_mate, half), sd_view(far_mate, half), sd_send.at[2 + i], sd_recv.at[2 + i], {"tp": mate}),
        )
        for i, half in enumerate((side_bit, 1 - side_bit))
    ]
    for copy in to_far[: 4 + EARLY]:
        copy.start()
    sd_to_far.start()
    for copy in to_far[4 + EARLY :]:
        copy.start()

    for i in (0, 1, 2, 3):
        loads[i].wait()
    mirrored = [
        remote(a, b, mirror_send.at[i], mirror_recv.at[i], {"ep": mirror})
        for i, (a, b) in enumerate(((choice, mirror_choice), (route, mirror_route)))
    ]

    @pl.when(middle_one == 1)
    def _():
        for copy in mirrored:
            copy.start()

    norm_into(own_rows, rows_in, 0, t * own, own, gain)
    lanes = rows_at(t * own, own, own)
    top = choice.shape[0]
    row_ids = lax.broadcasted_iota(jnp.int32, (slots // capacity, own), 0)
    earlier = lax.broadcasted_iota(jnp.int32, (own, own), 0)
    later = lax.broadcasted_iota(jnp.int32, (own, own), 1)
    before = (earlier < later).astype(f32)

    def slots_of(choices):
        chosen = choices[:, lanes]
        named = [row_ids == chosen[k : k + 1, :] for k in range(top)]
        named_any = functools.reduce(jnp.logical_or, named).astype(f32)
        ranks = jnp.dot(named_any, before, preferred_element_type=f32)
        return [
            chosen[k : k + 1, :] * capacity
            + jnp.sum(jnp.where(named[k], ranks, 0.0), axis=0, keepdims=True).astype(jnp.int32)
            for k in range(top)
        ]

    def column_of(row):
        return jnp.broadcast_to(row.astype(f32), (own, own)).T

    slot_rows = slots_of(choice)
    slot_ids = lax.broadcasted_iota(jnp.int32, (slots, own), 0)
    spread = functools.reduce(jnp.logical_or, [slot_ids == row for row in slot_rows])
    spread = spread.astype(f32).astype(bf16)
    for c in range(BLOCKS):
        cols = pl.ds(c * block, block)
        slots_out[:, cols] = jnp.dot(spread, own_rows[:, cols], preferred_element_type=f32).astype(bf16)

    def slot_block(ref, owner):
        return ref.at[rows_at(owner * capacity, capacity, capacity)]

    def slot_copy(k, target, origin):
        return remote(
            slot_block(slots_out, target), slot_block(slots_in, origin),
            slot_send.at[k], slot_recv.at[k], {"ep": target},
        )

    rows_copy = remote(own_rows, mirror_rows, row_send, row_recv, {"ep": mirror})

    def send_slots(side, k):
        target = (me + k) % ep_count

        @pl.when(target // (2 * quarter_size) == side)
        def _():
            slot_copy(k, target, me).start()

    def send_near(k, carry):
        send_slots(high, k)
        return carry

    def send_far(k, carry):
        send_slots(1 - high, k)
        return carry

    lax.fori_loop(1, ep_count, send_near, 0)

    for i in range(4, 9):
        loads[i].wait()
    pair = 2 * HEAD_DIM
    lane = lax.broadcasted_iota(jnp.int32, (1, pair), 1)
    first_half = lane % HEAD_DIM < HEAD_DIM // 2
    lower = lane < HEAD_DIM
    twice = lax.broadcasted_iota(jnp.int32, (HEAD_DIM, pair), 0)
    twice = (lax.broadcasted_iota(jnp.int32, (HEAD_DIM, pair), 1) % HEAD_DIM == twice).astype(f32).astype(bf16)
    first_position = me % (ep_count // SEQS) * tokens
    transposed = (((1,), (1,)), ((), ()))

    def turn(heads, rows):
        swapped = jnp.where(
            first_half,
            pltpu.roll(heads, pair - HEAD_DIM // 2, 1),
            pltpu.roll(heads, HEAD_DIM // 2, 1),
        )
        return heads * cosines[rows, :] + swapped * sines[rows, :]

    def project_keys(i, carry):
        rows = rows_at(i * WINDOW, WINDOW, WINDOW)
        after = rows_at((i + 1) * WINDOW, WINDOW, WINDOW)
        norm_into(normed, mixer_in, i * WINDOW, i * WINDOW, WINDOW, mixer_gain)
        position = lax.broadcasted_iota(jnp.int32, (WINDOW, pair), 0) + (first_position + i * WINDOW)
        angles = position.astype(f32) * freq[...]
        sine = jnp.sin(angles)
        cosines[rows, :] = jnp.cos(angles)
        sines[rows, :] = jnp.where(first_half, -sine, sine)
        source = normed[rows, :]
        keys = lax.dot_general(source, wk[...], transposed, preferred_element_type=f32).astype(bf16)
        keys = jnp.dot(keys, twice, preferred_element_type=f32)
        band[0, after, :] = turn(keys, rows).astype(bf16)
        values = lax.dot_general(source, wv[...], transposed, preferred_element_type=f32).astype(bf16)
        band[1, after, :] = jnp.dot(values, twice, preferred_element_type=f32).astype(bf16)
        return carry

    def halo_copy(target):
        return remote(
            band.at[:, pl.ds(tokens, WINDOW)], band.at[:, pl.ds(0, WINDOW)],
            halo_send, halo_recv, {"ep": target},
        )

    last_block = tokens // WINDOW - 1
    project_keys(last_block, 0)
    halo_copy((me + 1) % ep_count).start()

    @pl.when(middle_one == 1)
    def _():
        rows_copy.start()

    for copy in to_mate + sd_to_mate:
        copy.start()

    own_block = rows_at(me * capacity, capacity, capacity)
    slots_in[own_block, :] = slots_out[own_block, :]
    lane_ids = lax.broadcasted_iota(jnp.int32, (own, slots), 1)
    for k in range(top):
        picks[k] = (lane_ids == column_of(slot_rows[k])[:, :1].astype(jnp.int32)).astype(f32).astype(bf16)
        weights_col[k] = column_of(route[k : k + 1, lanes])

    @pl.when(middle_one == 1)
    def _():
        for c in range(PIECES):
            back[c, rows_at((1 - high) * side_rows, side_rows, capacity), :] = jnp.zeros((side_rows, piece), bf16)

    @pl.when(middle_one == 0)
    def _():
        dense_in[...] = jnp.zeros(dense_in.shape, bf16)

    half_copy = remote(mixer_part.at[1 - parity], half_in, half_send, half_recv, {"tp": mate})
    last_copy = remote(half_out, last_in, last_send, last_recv, {"tp": far})

    lax.fori_loop(0, last_block, project_keys, 0)
    loads[9].wait()
    pairs = wq.shape[1] // pair

    def project(i, carry):
        rows = rows_at(i * WINDOW, WINDOW, WINDOW)
        for j in range(pairs):
            cols = pl.ds(j * pair, pair)
            heads = jnp.dot(normed[rows, :], wq[:, cols], preferred_element_type=f32)
            turned_heads = turn(heads.astype(bf16).astype(f32), rows).astype(bf16)
            queries[rows, cols] = (turned_heads.astype(f32) * HEAD_DIM ** -0.5).astype(bf16)
        return carry

    lax.fori_loop(0, tokens // WINDOW, project, 0)

    norm_into(normed, rows_in, 0, 0, tokens, gain)
    for i in (11, 12):
        loads[i].wait()
    for r in range(2):
        rows = pl.ds(r * (tokens // 2), tokens // 2)
        gate = jnp.dot(normed[rows, :], sg[...], preferred_element_type=f32)
        up = jnp.dot(normed[rows, :], su[...], preferred_element_type=f32)
        shared_hidden[rows, :] = silu_times(gate, up).astype(bf16)

    def hid_copy(i, device, origin):
        return remote(
            shared_hidden.at[rows_at(device * own, own, own)],
            shared_all.at[:, rows_at(origin * shared_ff, shared_ff, shared_ff)],
            hid_send.at[i], hid_recv.at[i], {"tp": device},
        )

    hid_out = [hid_copy(i, device, t) for i, device in enumerate((mate, far, far_mate))]
    hid_in = [hid_copy(i, device, device) for i, device in enumerate((mate, far, far_mate))]
    for copy in hid_out:
        copy.start()
    shared_all[:, rows_at(t * shared_ff, shared_ff, shared_ff)] = shared_hidden[rows_at(t * own, own, own), :]

    @pl.when(middle_one == 0)
    def _():
        lax.fori_loop(1, ep_count, send_far, 0)

    for i in (10, 13):
        loads[i].wait()
    halo_copy((me + 1) % ep_count).wait_recv()
    count = 2 * pairs
    row = lax.broadcasted_iota(jnp.int32, (WINDOW, 2 * WINDOW), 0)
    key = lax.broadcasted_iota(jnp.int32, (WINDOW, 2 * WINDOW), 1)
    distance = row + WINDOW - key
    in_window = (distance >= 0) & (distance < WINDOW)

    for head in range(count):
        sunk[pl.ds(head * WINDOW, WINDOW), :] = jnp.broadcast_to(sink[:, head : head + 1], (WINDOW, pair))

    def attend(i, carry):
        rows = rows_at(i * WINDOW, WINDOW, WINDOW)
        reach = rows_at(i * WINDOW, 2 * WINDOW, WINDOW)
        allowed = in_window & (key + (first_position + (i - 1) * WINDOW) >= 0)
        both = [queries[rows, pl.ds(j * pair, pair)] for j in range(pairs)]
        none = jnp.zeros((WINDOW, pair), bf16)
        kept = jnp.concatenate(
            [jnp.where(side, heads, none) for heads in both for side in (lower, ~lower)], axis=0
        )
        scores = lax.dot_general(kept, band[0, reach, :], transposed, preferred_element_type=f32)
        scores = jnp.where(allowed[None], scores.reshape(count, WINDOW, 2 * WINDOW), -jnp.inf)
        scores = scores.reshape(count * WINDOW, 2 * WINDOW)
        sinks = sunk[:, :1]
        peak = jnp.maximum(jnp.max(scores, axis=-1, keepdims=True), sinks)
        raised = jnp.exp(scores - peak).astype(bf16)
        values = jnp.concatenate([band[1, reach, :], jnp.ones((2 * WINDOW, pair), bf16)], axis=1)
        mixed = jnp.dot(raised, values, preferred_element_type=f32)
        mixed = (mixed[:, :pair] / (mixed[:, pair:] + jnp.exp(sinks - peak))).reshape(count, WINDOW, pair)
        for j in range(pairs):
            attended[rows, pl.ds(j * pair, pair)] = jnp.where(
                lower, mixed[2 * j], mixed[2 * j + 1]
            ).astype(bf16)
        return carry

    lax.fori_loop(0, tokens // WINDOW, attend, 0)
    for owner in range(4):
        for c in range(BLOCKS):
            cols = pl.ds(c * block, block)
            mixer_part[owner % 2, owner // 2, :, cols] = jnp.dot(
                attended[pl.ds(owner * own, own), :], wo[:, cols], preferred_element_type=f32
            ).astype(bf16)
    half_copy.start()
    def dealt_copy(n):
        target = high * 2 * quarter_size + n
        return remote(
            slot_block(mirror_slots, n), slot_block(slots_in, mirror),
            dealt_send.at[n], slot_recv.at[(target - mirror + ep_count) % ep_count], {"ep": target},
        )

    my_place = (quarter % 2) * quarter_size + seat

    @pl.when(middle_one == 1)
    def _():
        for copy in mirrored:
            copy.wait_recv()
        mirror_slot_rows = slots_of(mirror_choice)
        near_ids = lax.broadcasted_iota(jnp.int32, (own, side_rows), 1) + high * side_rows
        for k, row in enumerate(mirror_slot_rows):
            mirror_picks[k] = (near_ids == column_of(row)[:, :1].astype(jnp.int32)).astype(f32).astype(bf16)
            mirror_weights[k] = column_of(mirror_route[k : k + 1, lanes])
        rows_copy.wait_recv()
        side_ids = lax.broadcasted_iota(jnp.int32, (side_rows, own), 0) + high * side_rows
        spread_side = functools.reduce(jnp.logical_or, [side_ids == row for row in mirror_slot_rows])
        spread_side = spread_side.astype(f32).astype(bf16)
        for c in range(BLOCKS):
            cols = pl.ds(c * block, block)
            mirror_slots[:, cols] = jnp.dot(
                spread_side, mirror_rows[:, cols], preferred_element_type=f32
            ).astype(bf16)

        def deal(n, carry):
            @pl.when(n != my_place)
            def _():
                dealt_copy(n).start()

            return carry

        lax.fori_loop(0, 2 * quarter_size, deal, 0)
        slots_in[rows_at(mirror * capacity, capacity, capacity), :] = mirror_slots[
            rows_at(my_place * capacity, capacity, capacity), :
        ]

    half_copy.wait_recv()
    half_out[...] = (mixer_part[parity, 1 - level].astype(f32) + half_in[1 - level].astype(f32)).astype(bf16)
    last_copy.start()

    def hidden_block(owner, side, half):
        rows = rows_at(side * side_rows, side_rows, capacity)
        weights = jnp.concatenate([wgu[owner, 2 * half], wgu[owner, 2 * half + 1]], axis=1)
        both = jnp.dot(slots_in[rows, :], weights, preferred_element_type=f32)
        hidden[rows, rows_at(owner * ff + half * part, part, part)] = silu_times(
            both[:, :part], both[:, part:]
        ).astype(bf16)

    def pass_on(i):
        from_far[i].wait_recv()
        to_pass[i].start()

    pass_on(0)

    def wait_slots(side):
        def wait_one(k, carry):
            source = (me + ep_count - k) % ep_count

            @pl.when((source // (2 * quarter_size) == side) & (middle_one * (source == mirror) == 0))
            def _():
                slot_copy(k, me, source).wait_recv()

            return carry

        lax.fori_loop(1, ep_count, wait_one, 0)

    wait_slots(high)
    for i in range(14, 20 + PIECES):
        loads[i].wait()
    for half in range(2):
        hidden_block(t, high, half)
    for copy in from_mate:
        copy.wait_recv()
    for half in range(2):
        hidden_block(mate, high, half)
    pass_on(1)
    hidden_block(far, high, 0)
    pass_on(2)
    for i in (0, 1):
        from_pass[i].wait_recv()
    hidden_block(far_mate, high, 0)
    wait_slots(1 - high)
    for half in range(2):
        hidden_block(t, 1 - high, half)
        hidden_block(mate, 1 - high, half)
    hidden_block(far, 1 - high, 0)
    hidden_block(far_mate, 1 - high, 0)
    pass_on(3)
    for side in range(2):
        hidden_block(far, side, 1)
    pass_on(4)
    for i in (2, 3):
        from_pass[i].wait_recv()
    for side in range(2):
        hidden_block(far_mate, side, 1)

    def is_low_middle(q):
        return (q % 2) * (1 - q // 2)

    def is_high_middle(q):
        return (q // 2) * (1 - q % 2)

    def turned(source, target):
        return is_low_middle(target) * (source // 2) + is_high_middle(target) * (1 - source // 2)

    def landing(source, source_seat, target):
        stop = turned(source, target)
        straight = source * quarter_size + source_seat
        return (1 - stop) * straight + stop * (ep_count + (source % 2) * quarter_size + source_seat)

    def back_copy(k, c, owner, target, block):
        cols = pl.ds(c * piece, piece)
        return remote(
            slot_block(result.at[c], owner), slot_block(back.at[c], block),
            back_send.at[k, c], back_recv.at[block, c], {"ep": target},
        )

    def each_back(c, remote_do, local_do):
        for n, q in enumerate((1, 0, 2, 3)):
            target = high * q + (1 - high) * (3 - q)
            stop = turned(quarter, target)
            via = target + stop * (2 * high - 1)

            def step(j, carry, n=n, target=target, via=via):
                to_seat = (seat + j) % quarter_size
                owner = target * quarter_size + to_seat
                device = via * quarter_size + to_seat
                block = landing(quarter, seat, target)

                @pl.when(device != me)
                def _():
                    remote_do(back_copy(n * quarter_size + j, c, owner, device, block))

                if local_do is not None:
                    @pl.when(device == me)
                    def _():
                        local_do(owner, block)

                return carry

            lax.fori_loop(0, quarter_size, step, 0)

    def wait_block(c, block):
        back_copy(0, c, me, me, block).wait_recv()

    def dense_copy(c):
        cols = pl.ds(c * piece, piece)
        return remote(
            dense_out.at[c], dense_in.at[c], dense_send.at[c], dense_recv.at[c], {"ep": mirror}
        )

    def relay(c):
        cols = pl.ds(c * piece, piece)

        @pl.when(middle_one == 1)
        def _():
            def wait_relayed(n, carry):
                @pl.when(n != (quarter % 2) * quarter_size + seat)
                def _():
                    wait_block(c, ep_count + n)

                return carry

            lax.fori_loop(0, 2 * quarter_size, wait_relayed, 0)
            total = 0.0
            for k in range(top):
                total = total + mirror_weights[k][:, :1] * jnp.dot(
                    mirror_picks[k], back[c, pl.ds(slots, side_rows), :], preferred_element_type=f32
                )
            dense_out[c] = total.astype(bf16)
            dense_copy(c).start()

    for c in range(PIECES):
        cols = pl.ds(c * piece, piece)
        from_pass[4 + c].wait_recv()
        result[c] = jnp.dot(hidden[...], wd[c], preferred_element_type=f32).astype(bf16)

        def keep(owner, block, c=c):
            back[c, rows_at(block * capacity, capacity, capacity), :] = result[
                c, rows_at(owner * capacity, capacity, capacity), :
            ]

        each_back(c, lambda copy: copy.start(), keep)
        if c + 1 == EARLY:
            sd_from_far.wait_recv()
            sd_to_beside.start()
            sd_passed[0][0].start()
        if c + 1 < PIECES:
            pass_on(5 + c)
        if c >= LAG:
            relay(c - LAG)
    for copy in to_far + to_mate + to_pass + hid_out + sd_to_mate:
        copy.wait_send()
    for copy in (sd_to_far, sd_to_beside, sd_passed[0][0], half_copy):
        copy.wait_send()

    @pl.when(middle_one == 1)
    def _():
        rows_copy.wait_send()
        for copy in mirrored:
            copy.wait_send()

        def dealt_done(n, carry):
            @pl.when(n != my_place)
            def _():
                dealt_copy(n).wait_send()

            return carry

        lax.fori_loop(0, 2 * quarter_size, dealt_done, 0)

    halo_copy((me + 1) % ep_count).wait_send()

    def drain(k, carry):
        target = (me + k) % ep_count
        other = target // (2 * quarter_size)

        @pl.when(middle_one * (other + high - 2 * other * high) == 0)
        def _():
            slot_copy(k, target, me).wait_send()

        return carry

    lax.fori_loop(1, ep_count, drain, 0)

    def back_done(c):
        each_back(c, lambda copy: copy.wait_send(), None)

        @pl.when(middle_one == 1)
        def _():
            dense_copy(c).wait_send()

    sd_from_beside.wait_recv()
    sd_passed[1][0].start()
    for c in range(PIECES - LAG, PIECES):
        relay(c)
    for copy in hid_in + sd_from_mate + [sd_passed[0][1]]:
        copy.wait_recv()
    sd_passed[1][1].wait_recv()
    for c in range(BLOCKS):
        cols = pl.ds(c * block, block)
        expert_sum[:, cols] = jnp.dot(shared_all[...], sd[c // (BLOCKS // 2), :, pl.ds(c % (BLOCKS // 2) * block, block)], preferred_element_type=f32)

    for c in range(PIECES):
        cols = pl.ds(c * piece, piece)

        def wait_back(k, carry, c=c):
            source = (me + ep_count - k) % ep_count

            @pl.when(turned(source // quarter_size, quarter) == 0)
            def _():
                wait_block(c, source)

            return carry

        lax.fori_loop(1, ep_count, wait_back, 0)

        @pl.when(middle_one == 1)
        def _(c=c):
            dense_copy(c).wait_recv()

        total = expert_sum[:, cols] + dense_in[c].astype(f32)
        for k in range(top):
            total = total + weights_col[k][:, :1] * jnp.dot(
                picks[k], back[c, pl.ds(0, slots), :], preferred_element_type=f32
            )
        expert_out[:, cols] = total
        if c >= LAG:
            back_done(c - LAG)
    last_copy.wait_recv()
    mixer_out[...] = mixer_part[parity, level].astype(f32) + half_in[level].astype(f32) + last_in[...].astype(f32)

    sd_passed[1][0].wait_send()
    last_copy.wait_send()
    for c in range(PIECES - LAG, PIECES):
        back_done(c)


def local(
    mixer_input,
    expert_input,
    gain_mixer,
    gain_expert,
    query_weight,
    key_weight,
    value_weight,
    sink_logits,
    output_weight,
    expert_choice,
    route_weights,
    expert_gate,
    expert_up,
    expert_down,
    shared_gate,
    shared_up,
    shared_down,
):
    tp_count = lax.axis_size("tp")
    ep_count = lax.axis_size("ep")
    tokens, width = expert_input.shape
    own = tokens // tp_count
    top = expert_choice.shape[1]
    local_experts, _, ff = expert_gate.shape
    shared_ff = shared_gate.shape[1]
    experts_all = local_experts * ep_count
    capacity = -(-(2 * own * top // experts_all) // 16) * 16
    slots = experts_all * capacity
    side_rows = slots // 2
    assert tp_count == 4 and local_experts == 1 and ep_count % 4 == 0
    heads = query_weight.shape[1] // HEAD_DIM
    assert heads % 2 == 0 and key_weight.shape[1] == HEAD_DIM and own % WINDOW == 0
    hbm_spec = pl.BlockSpec(memory_space=pltpu.HBM)
    vmem_spec = pl.BlockSpec(memory_space=pltpu.VMEM)
    dma = pltpu.SemaphoreType.DMA
    vmem = pltpu.VMEM
    piece = width // PIECES
    count = 4 + PIECES
    scratch = [
        vmem((tokens, width), bf16),
        vmem((tokens, width), bf16),
        vmem((1, width), f32),
        vmem((top, tokens), jnp.int32),
        vmem((top, tokens), f32),
        vmem((tp_count, 4, width, ff // 2), bf16),
        vmem((PIECES, tp_count * ff, piece), bf16),
        vmem((width, shared_ff), bf16),
        vmem((width, shared_ff), bf16),
        vmem((2, tp_count * shared_ff, width // 2), bf16),
        vmem((tokens, width), bf16),
        vmem((1, width), f32),
        vmem(query_weight.shape, bf16),
        vmem((HEAD_DIM, width), bf16),
        vmem((HEAD_DIM, width), bf16),
        vmem(output_weight.shape, bf16),
        vmem((1, heads), f32),
        vmem((heads * WINDOW, 2 * HEAD_DIM), f32),
        vmem((1, 2 * HEAD_DIM), f32),
        vmem((tokens, 2 * HEAD_DIM), f32),
        vmem((tokens, 2 * HEAD_DIM), f32),
        vmem((tokens, heads * HEAD_DIM), bf16),
        vmem((2, WINDOW + tokens, 2 * HEAD_DIM), bf16),
        vmem((tokens, heads * HEAD_DIM), bf16),
        vmem((own, width), bf16),
        vmem((slots, width), bf16),
        vmem((slots, width), bf16),
        vmem((slots, tp_count * ff), bf16),
        vmem((PIECES, slots, piece), bf16),
        vmem((PIECES, slots + side_rows, piece), bf16),
        vmem((top, own, slots), bf16),
        vmem((top, own, own), f32),
        vmem((top, tokens), jnp.int32),
        vmem((top, tokens), f32),
        vmem((top, own, side_rows), bf16),
        vmem((top, own, own), f32),
        vmem((PIECES, own, piece), bf16),
        vmem((PIECES, own, piece), bf16),
        vmem((own, width), f32),
        vmem((2, 2, own, width), bf16),
        vmem((tokens, shared_ff), bf16),
        vmem((own, tp_count * shared_ff), bf16),
        vmem((2, own, width), bf16),
        vmem((own, width), bf16),
        vmem((own, width), bf16),
        vmem((own, width), bf16),
        vmem((side_rows, width), bf16),
        dma((20 + PIECES,)),
        dma((count,)), dma((count,)),
        dma((count,)), dma((count,)),
        dma((count,)), dma((count,)),
        dma((ep_count,)), dma((ep_count,)),
        dma((ep_count, PIECES)), dma((ep_count + ep_count // 2, PIECES)),
        dma, dma,
        dma, dma,
        dma, dma,
        dma((2,)), dma((2,)),
        dma((PIECES,)), dma((PIECES,)),
        dma((ep_count // 2,)), dma, dma,
        dma((3,)), dma((3,)),
        dma((6,)), dma((6,)),
    ]
    sums = pl.pallas_call(
        functools.partial(mixture_kernel, capacity),
        out_shape=(jax.ShapeDtypeStruct((own, width), f32),) * 2,
        in_specs=[hbm_spec] * 18,
        out_specs=(vmem_spec,) * 2,
        scratch_shapes=scratch,
        compiler_params=pltpu.CompilerParams(
            collective_id=0, has_side_effects=True, vmem_limit_bytes=62 * 1024 * 1024
        ),
    )(
        expert_input, gain_expert[None, :], expert_choice.T, route_weights.T,
        expert_gate[0], expert_up[0], expert_down[0], shared_gate, shared_up, shared_down,
        mixer_input, gain_mixer[None, :], query_weight, key_weight.T, value_weight.T, output_weight,
        sink_logits[None, :], frequencies(HEAD_DIM),
    )
    def round_both(a_ref, b_ref, mixer_out, expert_out):
        mixer_out[...] = a_ref[...].astype(bf16)
        expert_out[...] = b_ref[...].astype(bf16)

    return pl.pallas_call(
        round_both,
        grid=(1,),
        out_shape=(jax.ShapeDtypeStruct((own, width), bf16),) * 2,
        in_specs=(pl.BlockSpec((own, width), lambda i: (i, 0)),) * 2,
        out_specs=(pl.BlockSpec((own, width), lambda i: (i, 0)),) * 2,
    )(*sums)


def solution(mesh):
    placed = (
        P("ep", None),
        P("ep", None),
        P(),
        P(),
        P(None, "tp"),
        P(None, "tp"),
        P(None, "tp"),
        P("tp"),
        P("tp", None),
        P("ep", None),
        P("ep", None),
        P("ep", None, "tp"),
        P("ep", None, "tp"),
        P("ep", "tp", None),
        P(None, "tp"),
        P(None, "tp"),
        P("tp", None),
    )
    return jax.shard_map(
        local,
        mesh=mesh,
        in_specs=placed,
        out_specs=(P(("ep", "tp"), None), P(("ep", "tp"), None)),
        check_vma=False,
    )
```

```python
import functools

import jax
import jax.numpy as jnp
import numpy as np
from jax import lax
from jax.experimental import pallas as pl
from jax.experimental.pallas import tpu as pltpu
from jax.sharding import PartitionSpec as P

HEAD_DIM = 64
WINDOW = 128
SEQS = 1
PIECES = 8
BLOCKS = 4
LAG = 2
EARLY = 6

norm_eps = 1e-06
rope_base = 500000.0
bf16 = jnp.bfloat16
f32 = jnp.float32
MESH = pl.DeviceIdType.MESH


def frequencies(head_size):
    half_steps = np.arange(head_size // 2, dtype=np.float64)
    return np.tile(rope_base ** (-(2.0 * half_steps) / head_size), 4).astype(np.float32)[None, :]


def rows_at(start, count, unit):
    return pl.ds(pl.multiple_of(start, unit), count)


def norm_into(target, source, to, start, count, gain):
    step = 32

    def body(i, carry):
        widened = source[rows_at(start + i * step, step, step), :].astype(f32)
        scale = lax.rsqrt(jnp.mean(widened * widened, axis=-1, keepdims=True) + norm_eps)
        target[rows_at(to + i * step, step, step), :] = (widened * scale * gain[...]).astype(bf16)
        return carry

    lax.fori_loop(0, count // step, body, 0)


def silu_times(gate, up):
    return gate / (1.0 + jnp.exp(-gate)) * up


def mixture_kernel(
    capacity,
    x_ref, gain_ref, choice_ref, route_ref,
    wg_ref, wu_ref, wd_ref, sg_ref, su_ref, sd_ref,
    mx_ref, mgain_ref, wq_ref, wk_ref, wv_ref, wo_ref, sink_ref, freq_ref,
    mixer_ref, expert_ref,
    rows_in, normed, gain, choice, route, wgu, wd, sg, su, sd,
    mixer_in, mixer_gain, wq, wk, wv, wo, sink, sunk, freq, cosines, sines, queries, band, attended,
    own_rows, slots_out, slots_in, hidden, result, back, picks, weights_col,
    mirror_choice, mirror_route, mirror_picks, mirror_weights, dense_out, dense_in, expert_sum, mixer_out, expert_out, out_sem,
    mixer_part, shared_hidden, shared_all, half_in, half_out, last_in, mirror_rows, mirror_slots,
    load_sem, far_send, far_recv, mate_send, mate_recv, pass_send, pass_recv,
    slot_send, slot_recv, back_send, back_recv, half_send, half_recv, last_send, last_recv,
    halo_send, halo_recv, mirror_send, mirror_recv, dense_send, dense_recv,
    dealt_send, row_send, row_recv, hid_send, hid_recv, sd_send, sd_recv,
):
    ep_count = lax.axis_size("ep")
    me = lax.axis_index("ep")
    t = lax.axis_index("tp")
    parity = t % 2
    level = t // 2
    mate = t + 1 - 2 * parity
    far = (t + 2) % 4
    far_mate = (mate + 2) % 4
    tokens, width = rows_in.shape
    own = own_rows.shape[0]
    quarter_size = ep_count // 4
    quarter = me // quarter_size
    seat = me % quarter_size
    high = quarter // 2
    middle_one = (quarter + high) % 2
    mirror = (3 - quarter) * quarter_size + seat
    side_rows = 2 * quarter_size * capacity
    ff = wd_ref.shape[0]
    shared_ff = sd_ref.shape[0]
    block = width // BLOCKS
    slots = slots_out.shape[0]
    piece = width // PIECES

    barrier = pltpu.get_barrier_semaphore()

    def greet(k, carry):
        pl.semaphore_signal(barrier, inc=1, device_id={"ep": (me + k) % ep_count}, device_id_type=MESH)
        return carry

    lax.fori_loop(1, ep_count, greet, 0)
    for other in (mate, far, far_mate):
        pl.semaphore_signal(barrier, inc=1, device_id={"tp": other}, device_id_type=MESH)

    part = ff // 2
    halves = [pl.ds(h * part, part) for h in range(2)]
    gate_up_sources = [ref.at[:, half] for half in halves for ref in (wg_ref, wu_ref)]
    sources = gate_up_sources + [wd_ref.at[:, pl.ds(c * piece, piece)] for c in range(PIECES)]

    def gate_up_views(owner):
        return [wgu.at[owner, i] for i in range(4)]

    wide = width // 2

    def sd_view(owner, half):
        return sd.at[half, rows_at(owner * shared_ff, shared_ff, shared_ff)]

    def block_views(owner):
        return gate_up_views(owner) + [wd.at[c, rows_at(owner * ff, ff, ff)] for c in range(PIECES)]

    loads = [
        (gain_ref, gain), (choice_ref, choice), (route_ref, route), (x_ref, rows_in),
        (mgain_ref, mixer_gain), (freq_ref, freq), (mx_ref, mixer_in), (wk_ref, wk), (wv_ref, wv),
        (wq_ref, wq), (sink_ref, sink), (sg_ref, sg), (su_ref, su), (wo_ref, wo),
    ]
    loads += [(sd_ref.at[:, pl.ds(h * wide, wide)], sd_view(t, h)) for h in range(2)]
    loads += list(zip(sources, block_views(t)))
    loads = [pltpu.make_async_copy(a, b, load_sem.at[i]) for i, (a, b) in enumerate(loads)]
    for load in loads:
        load.start()

    pl.semaphore_wait(barrier, ep_count + 2)

    def remote(src, dst, send, recv, device):
        return pltpu.make_async_remote_copy(
            src_ref=src, dst_ref=dst, send_sem=send, recv_sem=recv,
            device_id=device, device_id_type=MESH,
        )

    def views_copy(srcs, owner, send, recv, device):
        return [
            remote(a, b, send.at[i], recv.at[i], device)
            for i, (a, b) in enumerate(zip(srcs, block_views(owner)))
        ]

    to_far = views_copy(sources, t, far_send, far_recv, {"tp": far})
    to_mate = views_copy(sources, t, mate_send, mate_recv, {"tp": mate})
    from_far = views_copy(sources, far, far_send, far_recv, {"tp": far})
    from_mate = views_copy(sources, mate, mate_send, mate_recv, {"tp": mate})
    to_pass = views_copy(block_views(far), far, pass_send, pass_recv, {"tp": mate})
    from_pass = views_copy(block_views(far), far_mate, pass_send, pass_recv, {"tp": mate})
    side_bit = me % 2
    beside = me + 1 - 2 * side_bit
    sd_to_far = remote(
        sd_ref.at[:, rows_at(side_bit * wide, wide, wide)], sd_view(t, side_bit),
        sd_send.at[0], sd_recv.at[0], {"tp": far},
    )
    sd_from_far = remote(sd_view(far, side_bit), sd_view(far, side_bit), sd_send.at[0], sd_recv.at[0], {"tp": far})
    sd_to_beside = remote(sd_view(far, side_bit), sd_view(far, side_bit), sd_send.at[1], sd_recv.at[1], {"ep": beside})
    sd_from_beside = remote(sd_view(far, 1 - side_bit), sd_view(far, 1 - side_bit), sd_send.at[1], sd_recv.at[1], {"ep": beside})
    sd_to_mate, sd_from_mate = (
        [
            remote(sd_ref.at[:, pl.ds(h * wide, wide)], sd_view(owner, h), sd_send.at[4 + h], sd_recv.at[4 + h], {"tp": mate})
            for h in range(2)
        ]
        for owner in (t, mate)
    )
    sd_passed = [
        (
            remote(sd_view(far, half), sd_view(far, half), sd_send.at[2 + i], sd_recv.at[2 + i], {"tp": mate}),
            remote(sd_view(far_mate, half), sd_view(far_mate, half), sd_send.at[2 + i], sd_recv.at[2 + i], {"tp": mate}),
        )
        for i, half in enumerate((side_bit, 1 - side_bit))
    ]
    for copy in to_far[: 4 + EARLY]:
        copy.start()
    sd_to_far.start()
    for copy in to_far[4 + EARLY :]:
        copy.start()

    for i in (0, 1, 2, 3):
        loads[i].wait()
    mirrored = [
        remote(a, b, mirror_send.at[i], mirror_recv.at[i], {"ep": mirror})
        for i, (a, b) in enumerate(((choice, mirror_choice), (route, mirror_route)))
    ]

    @pl.when(middle_one == 1)
    def _():
        for copy in mirrored:
            copy.start()

    norm_into(own_rows, rows_in, 0, t * own, own, gain)
    lanes = rows_at(t * own, own, own)
    top = choice.shape[0]
    row_ids = lax.broadcasted_iota(jnp.int32, (slots // capacity, own), 0)
    earlier = lax.broadcasted_iota(jnp.int32, (own, own), 0)
    later = lax.broadcasted_iota(jnp.int32, (own, own), 1)
    before = (earlier < later).astype(f32)

    def slots_of(choices):
        chosen = choices[:, lanes]
        named = [row_ids == chosen[k : k + 1, :] for k in range(top)]
        named_any = functools.reduce(jnp.logical_or, named).astype(f32)
        ranks = jnp.dot(named_any, before, preferred_element_type=f32)
        return [
            chosen[k : k + 1, :] * capacity
            + jnp.sum(jnp.where(named[k], ranks, 0.0), axis=0, keepdims=True).astype(jnp.int32)
            for k in range(top)
        ]

    def column_of(row):
        return jnp.broadcast_to(row.astype(f32), (own, own)).T

    slot_rows = slots_of(choice)
    slot_ids = lax.broadcasted_iota(jnp.int32, (slots, own), 0)
    spread = functools.reduce(jnp.logical_or, [slot_ids == row for row in slot_rows])
    spread = spread.astype(f32).astype(bf16)
    for c in range(BLOCKS):
        cols = pl.ds(c * block, block)
        slots_out[:, cols] = jnp.dot(spread, own_rows[:, cols], preferred_element_type=f32).astype(bf16)

    def slot_block(ref, owner):
        return ref.at[rows_at(owner * capacity, capacity, capacity)]

    def slot_copy(k, target, origin):
        return remote(
            slot_block(slots_out, target), slot_block(slots_in, origin),
            slot_send.at[k], slot_recv.at[k], {"ep": target},
        )

    rows_copy = remote(own_rows, mirror_rows, row_send, row_recv, {"ep": mirror})

    def send_slots(side, k):
        target = (me + k) % ep_count

        @pl.when(target // (2 * quarter_size) == side)
        def _():
            slot_copy(k, target, me).start()

    def send_near(k, carry):
        send_slots(high, k)
        return carry

    def send_far(k, carry):
        send_slots(1 - high, k)
        return carry

    lax.fori_loop(1, ep_count, send_near, 0)

    for i in range(4, 9):
        loads[i].wait()
    pair = 2 * HEAD_DIM
    lane = lax.broadcasted_iota(jnp.int32, (1, pair), 1)
    first_half = lane % HEAD_DIM < HEAD_DIM // 2
    lower = lane < HEAD_DIM
    twice = lax.broadcasted_iota(jnp.int32, (HEAD_DIM, pair), 0)
    twice = (lax.broadcasted_iota(jnp.int32, (HEAD_DIM, pair), 1) % HEAD_DIM == twice).astype(f32).astype(bf16)
    first_position = me % (ep_count // SEQS) * tokens
    transposed = (((1,), (1,)), ((), ()))

    def turn(heads, rows):
        swapped = jnp.where(
            first_half,
            pltpu.roll(heads, pair - HEAD_DIM // 2, 1),
            pltpu.roll(heads, HEAD_DIM // 2, 1),
        )
        return heads * cosines[rows, :] + swapped * sines[rows, :]

    def project_keys(i, carry):
        rows = rows_at(i * WINDOW, WINDOW, WINDOW)
        after = rows_at((i + 1) * WINDOW, WINDOW, WINDOW)
        norm_into(normed, mixer_in, i * WINDOW, i * WINDOW, WINDOW, mixer_gain)
        position = lax.broadcasted_iota(jnp.int32, (WINDOW, pair), 0) + (first_position + i * WINDOW)
        angles = position.astype(f32) * freq[...]
        sine = jnp.sin(angles)
        cosines[rows, :] = jnp.cos(angles)
        sines[rows, :] = jnp.where(first_half, -sine, sine)
        source = normed[rows, :]
        keys = lax.dot_general(source, wk[...], transposed, preferred_element_type=f32).astype(bf16)
        keys = jnp.dot(keys, twice, preferred_element_type=f32)
        band[0, after, :] = turn(keys, rows).astype(bf16)
        values = lax.dot_general(source, wv[...], transposed, preferred_element_type=f32).astype(bf16)
        band[1, after, :] = jnp.dot(values, twice, preferred_element_type=f32).astype(bf16)
        return carry

    def halo_copy(target):
        return remote(
            band.at[:, pl.ds(tokens, WINDOW)], band.at[:, pl.ds(0, WINDOW)],
            halo_send, halo_recv, {"ep": target},
        )

    last_block = tokens // WINDOW - 1
    project_keys(last_block, 0)
    halo_copy((me + 1) % ep_count).start()

    @pl.when(middle_one == 1)
    def _():
        rows_copy.start()

    for copy in to_mate + sd_to_mate:
        copy.start()

    own_block = rows_at(me * capacity, capacity, capacity)
    slots_in[own_block, :] = slots_out[own_block, :]
    lane_ids = lax.broadcasted_iota(jnp.int32, (own, slots), 1)
    for k in range(top):
        picks[k] = (lane_ids == column_of(slot_rows[k])[:, :1].astype(jnp.int32)).astype(f32).astype(bf16)
        weights_col[k] = column_of(route[k : k + 1, lanes])

    @pl.when(middle_one == 1)
    def _():
        for c in range(PIECES):
            back[c, rows_at((1 - high) * side_rows, side_rows, capacity), :] = jnp.zeros((side_rows, piece), bf16)

    @pl.when(middle_one == 0)
    def _():
        dense_in[...] = jnp.zeros(dense_in.shape, bf16)

    half_copy = remote(mixer_part.at[1 - parity], half_in, half_send, half_recv, {"tp": mate})
    last_copy = remote(half_out, last_in, last_send, last_recv, {"tp": far})

    lax.fori_loop(0, last_block, project_keys, 0)
    loads[9].wait()
    pairs = wq.shape[1] // pair

    def project(i, carry):
        rows = rows_at(i * WINDOW, WINDOW, WINDOW)
        for j in range(pairs):
            cols = pl.ds(j * pair, pair)
            heads = jnp.dot(normed[rows, :], wq[:, cols], preferred_element_type=f32)
            turned_heads = turn(heads.astype(bf16).astype(f32), rows).astype(bf16)
            queries[rows, cols] = (turned_heads.astype(f32) * HEAD_DIM ** -0.5).astype(bf16)
        return carry

    lax.fori_loop(0, tokens // WINDOW, project, 0)

    norm_into(normed, rows_in, 0, 0, tokens, gain)
    for i in (11, 12):
        loads[i].wait()
    for r in range(2):
        rows = pl.ds(r * (tokens // 2), tokens // 2)
        gate = jnp.dot(normed[rows, :], sg[...], preferred_element_type=f32)
        up = jnp.dot(normed[rows, :], su[...], preferred_element_type=f32)
        shared_hidden[rows, :] = silu_times(gate, up).astype(bf16)

    def hid_copy(i, device, origin):
        return remote(
            shared_hidden.at[rows_at(device * own, own, own)],
            shared_all.at[:, rows_at(origin * shared_ff, shared_ff, shared_ff)],
            hid_send.at[i], hid_recv.at[i], {"tp": device},
        )

    hid_out = [hid_copy(i, device, t) for i, device in enumerate((mate, far, far_mate))]
    hid_in = [hid_copy(i, device, device) for i, device in enumerate((mate, far, far_mate))]
    for copy in hid_out:
        copy.start()
    shared_all[:, rows_at(t * shared_ff, shared_ff, shared_ff)] = shared_hidden[rows_at(t * own, own, own), :]

    @pl.when(middle_one == 0)
    def _():
        lax.fori_loop(1, ep_count, send_far, 0)

    for i in (10, 13):
        loads[i].wait()
    halo_copy((me + 1) % ep_count).wait_recv()
    count = 2 * pairs
    row = lax.broadcasted_iota(jnp.int32, (WINDOW, 2 * WINDOW), 0)
    key = lax.broadcasted_iota(jnp.int32, (WINDOW, 2 * WINDOW), 1)
    distance = row + WINDOW - key
    in_window = (distance >= 0) & (distance < WINDOW)

    for head in range(count):
        sunk[pl.ds(head * WINDOW, WINDOW), :] = jnp.broadcast_to(sink[:, head : head + 1], (WINDOW, pair))

    def attend(i, carry):
        rows = rows_at(i * WINDOW, WINDOW, WINDOW)
        reach = rows_at(i * WINDOW, 2 * WINDOW, WINDOW)
        allowed = in_window & (key + (first_position + (i - 1) * WINDOW) >= 0)
        both = [queries[rows, pl.ds(j * pair, pair)] for j in range(pairs)]
        none = jnp.zeros((WINDOW, pair), bf16)
        kept = jnp.concatenate(
            [jnp.where(side, heads, none) for heads in both for side in (lower, ~lower)], axis=0
        )
        scores = lax.dot_general(kept, band[0, reach, :], transposed, preferred_element_type=f32)
        scores = jnp.where(allowed[None], scores.reshape(count, WINDOW, 2 * WINDOW), -jnp.inf)
        scores = scores.reshape(count * WINDOW, 2 * WINDOW)
        sinks = sunk[:, :1]
        peak = jnp.maximum(jnp.max(scores, axis=-1, keepdims=True), sinks)
        raised = jnp.exp(scores - peak).astype(bf16)
        values = jnp.concatenate([band[1, reach, :], jnp.ones((2 * WINDOW, pair), bf16)], axis=1)
        mixed = jnp.dot(raised, values, preferred_element_type=f32)
        mixed = (mixed[:, :pair] / (mixed[:, pair:] + jnp.exp(sinks - peak))).reshape(count, WINDOW, pair)
        for j in range(pairs):
            attended[rows, pl.ds(j * pair, pair)] = jnp.where(
                lower, mixed[2 * j], mixed[2 * j + 1]
            ).astype(bf16)
        return carry

    lax.fori_loop(0, tokens // WINDOW, attend, 0)
    for owner in range(4):
        for c in range(BLOCKS):
            cols = pl.ds(c * block, block)
            mixer_part[owner % 2, owner // 2, :, cols] = jnp.dot(
                attended[pl.ds(owner * own, own), :], wo[:, cols], preferred_element_type=f32
            ).astype(bf16)
    half_copy.start()
    def dealt_copy(n):
        target = high * 2 * quarter_size + n
        return remote(
            slot_block(mirror_slots, n), slot_block(slots_in, mirror),
            dealt_send.at[n], slot_recv.at[(target - mirror + ep_count) % ep_count], {"ep": target},
        )

    my_place = (quarter % 2) * quarter_size + seat

    @pl.when(middle_one == 1)
    def _():
        for copy in mirrored:
            copy.wait_recv()
        mirror_slot_rows = slots_of(mirror_choice)
        near_ids = lax.broadcasted_iota(jnp.int32, (own, side_rows), 1) + high * side_rows
        for k, row in enumerate(mirror_slot_rows):
            mirror_picks[k] = (near_ids == column_of(row)[:, :1].astype(jnp.int32)).astype(f32).astype(bf16)
            mirror_weights[k] = column_of(mirror_route[k : k + 1, lanes])
        rows_copy.wait_recv()
        side_ids = lax.broadcasted_iota(jnp.int32, (side_rows, own), 0) + high * side_rows
        spread_side = functools.reduce(jnp.logical_or, [side_ids == row for row in mirror_slot_rows])
        spread_side = spread_side.astype(f32).astype(bf16)
        for c in range(BLOCKS):
            cols = pl.ds(c * block, block)
            mirror_slots[:, cols] = jnp.dot(
                spread_side, mirror_rows[:, cols], preferred_element_type=f32
            ).astype(bf16)

        def deal(n, carry):
            @pl.when(n != my_place)
            def _():
                dealt_copy(n).start()

            return carry

        lax.fori_loop(0, 2 * quarter_size, deal, 0)
        slots_in[rows_at(mirror * capacity, capacity, capacity), :] = mirror_slots[
            rows_at(my_place * capacity, capacity, capacity), :
        ]

    half_copy.wait_recv()
    half_out[...] = (mixer_part[parity, 1 - level].astype(f32) + half_in[1 - level].astype(f32)).astype(bf16)
    last_copy.start()

    def hidden_block(owner, side, half):
        rows = rows_at(side * side_rows, side_rows, capacity)
        weights = jnp.concatenate([wgu[owner, 2 * half], wgu[owner, 2 * half + 1]], axis=1)
        both = jnp.dot(slots_in[rows, :], weights, preferred_element_type=f32)
        hidden[rows, rows_at(owner * ff + half * part, part, part)] = silu_times(
            both[:, :part], both[:, part:]
        ).astype(bf16)

    def pass_on(i):
        from_far[i].wait_recv()
        to_pass[i].start()

    pass_on(0)

    def wait_slots(side):
        def wait_one(k, carry):
            source = (me + ep_count - k) % ep_count

            @pl.when((source // (2 * quarter_size) == side) & (middle_one * (source == mirror) == 0))
            def _():
                slot_copy(k, me, source).wait_recv()

            return carry

        lax.fori_loop(1, ep_count, wait_one, 0)

    wait_slots(high)
    for i in range(14, 20 + PIECES):
        loads[i].wait()
    for half in range(2):
        hidden_block(t, high, half)
    for copy in from_mate:
        copy.wait_recv()
    for half in range(2):
        hidden_block(mate, high, half)
    pass_on(1)
    hidden_block(far, high, 0)
    pass_on(2)
    for i in (0, 1):
        from_pass[i].wait_recv()
    hidden_block(far_mate, high, 0)
    wait_slots(1 - high)
    for half in range(2):
        hidden_block(t, 1 - high, half)
        hidden_block(mate, 1 - high, half)
    hidden_block(far, 1 - high, 0)
    hidden_block(far_mate, 1 - high, 0)
    pass_on(3)
    for side in range(2):
        hidden_block(far, side, 1)
    pass_on(4)
    for i in (2, 3):
        from_pass[i].wait_recv()
    for side in range(2):
        hidden_block(far_mate, side, 1)

    def is_low_middle(q):
        return (q % 2) * (1 - q // 2)

    def is_high_middle(q):
        return (q // 2) * (1 - q % 2)

    def turned(source, target):
        return is_low_middle(target) * (source // 2) + is_high_middle(target) * (1 - source // 2)

    def landing(source, source_seat, target):
        stop = turned(source, target)
        straight = source * quarter_size + source_seat
        return (1 - stop) * straight + stop * (ep_count + (source % 2) * quarter_size + source_seat)

    def back_copy(k, c, owner, target, block):
        cols = pl.ds(c * piece, piece)
        return remote(
            slot_block(result.at[c], owner), slot_block(back.at[c], block),
            back_send.at[k, c], back_recv.at[block, c], {"ep": target},
        )

    def each_back(c, remote_do, local_do):
        for n, q in enumerate((1, 0, 2, 3)):
            target = high * q + (1 - high) * (3 - q)
            stop = turned(quarter, target)
            via = target + stop * (2 * high - 1)

            def step(j, carry, n=n, target=target, via=via):
                to_seat = (seat + j) % quarter_size
                owner = target * quarter_size + to_seat
                device = via * quarter_size + to_seat
                block = landing(quarter, seat, target)

                @pl.when(device != me)
                def _():
                    remote_do(back_copy(n * quarter_size + j, c, owner, device, block))

                if local_do is not None:
                    @pl.when(device == me)
                    def _():
                        local_do(owner, block)

                return carry

            lax.fori_loop(0, quarter_size, step, 0)

    def wait_block(c, block):
        back_copy(0, c, me, me, block).wait_recv()

    def dense_copy(c):
        cols = pl.ds(c * piece, piece)
        return remote(
            dense_out.at[c], dense_in.at[c], dense_send.at[c], dense_recv.at[c], {"ep": mirror}
        )

    def relay(c):
        cols = pl.ds(c * piece, piece)

        @pl.when(middle_one == 1)
        def _():
            def wait_relayed(n, carry):
                @pl.when(n != (quarter % 2) * quarter_size + seat)
                def _():
                    wait_block(c, ep_count + n)

                return carry

            lax.fori_loop(0, 2 * quarter_size, wait_relayed, 0)
            total = 0.0
            for k in range(top):
                total = total + mirror_weights[k][:, :1] * jnp.dot(
                    mirror_picks[k], back[c, pl.ds(slots, side_rows), :], preferred_element_type=f32
                )
            dense_out[c] = total.astype(bf16)
            dense_copy(c).start()

    for c in range(PIECES):
        cols = pl.ds(c * piece, piece)
        from_pass[4 + c].wait_recv()
        result[c] = jnp.dot(hidden[...], wd[c], preferred_element_type=f32).astype(bf16)

        def keep(owner, block, c=c):
            back[c, rows_at(block * capacity, capacity, capacity), :] = result[
                c, rows_at(owner * capacity, capacity, capacity), :
            ]

        each_back(c, lambda copy: copy.start(), keep)
        if c + 1 == EARLY:
            sd_from_far.wait_recv()
            sd_to_beside.start()
            sd_passed[0][0].start()
        if c + 1 < PIECES:
            pass_on(5 + c)
        if c >= LAG:
            relay(c - LAG)
    for copy in to_far + to_mate + to_pass + hid_out + sd_to_mate:
        copy.wait_send()
    for copy in (sd_to_far, sd_to_beside, sd_passed[0][0], half_copy):
        copy.wait_send()

    @pl.when(middle_one == 1)
    def _():
        rows_copy.wait_send()
        for copy in mirrored:
            copy.wait_send()

        def dealt_done(n, carry):
            @pl.when(n != my_place)
            def _():
                dealt_copy(n).wait_send()

            return carry

        lax.fori_loop(0, 2 * quarter_size, dealt_done, 0)

    halo_copy((me + 1) % ep_count).wait_send()

    def drain(k, carry):
        target = (me + k) % ep_count
        other = target // (2 * quarter_size)

        @pl.when(middle_one * (other + high - 2 * other * high) == 0)
        def _():
            slot_copy(k, target, me).wait_send()

        return carry

    lax.fori_loop(1, ep_count, drain, 0)

    def back_done(c):
        each_back(c, lambda copy: copy.wait_send(), None)

        @pl.when(middle_one == 1)
        def _():
            dense_copy(c).wait_send()

    sd_from_beside.wait_recv()
    sd_passed[1][0].start()
    for c in range(PIECES - LAG, PIECES):
        relay(c)
    for copy in hid_in + sd_from_mate + [sd_passed[0][1]]:
        copy.wait_recv()
    sd_passed[1][1].wait_recv()
    for c in range(BLOCKS):
        cols = pl.ds(c * block, block)
        expert_sum[:, cols] = jnp.dot(shared_all[...], sd[c // (BLOCKS // 2), :, pl.ds(c % (BLOCKS // 2) * block, block)], preferred_element_type=f32)

    mixer_copy = pltpu.make_async_copy(mixer_out, mixer_ref, out_sem.at[PIECES])

    def expert_copy(c):
        return pltpu.make_async_copy(
            expert_out.at[c], expert_ref.at[:, pl.ds(c * piece, piece)], out_sem.at[c]
        )

    for c in range(PIECES):
        cols = pl.ds(c * piece, piece)

        def wait_back(k, carry, c=c):
            source = (me + ep_count - k) % ep_count

            @pl.when(turned(source // quarter_size, quarter) == 0)
            def _():
                wait_block(c, source)

            return carry

        lax.fori_loop(1, ep_count, wait_back, 0)

        @pl.when(middle_one == 1)
        def _(c=c):
            dense_copy(c).wait_recv()

        total = expert_sum[:, cols] + dense_in[c].astype(f32)
        for k in range(top):
            total = total + weights_col[k][:, :1] * jnp.dot(
                picks[k], back[c, pl.ds(0, slots), :], preferred_element_type=f32
            )
        expert_out[c] = total.astype(bf16)
        expert_copy(c).start()
        if c == PIECES - 2:
            last_copy.wait_recv()
            mixer_sum = mixer_part[parity, level].astype(f32) + half_in[level].astype(f32)
            mixer_out[...] = (mixer_sum + last_in[...].astype(f32)).astype(bf16)
            mixer_copy.start()
        if c >= LAG:
            back_done(c - LAG)

    sd_passed[1][0].wait_send()
    last_copy.wait_send()
    for c in range(PIECES - LAG, PIECES):
        back_done(c)
    mixer_copy.wait()
    for c in range(PIECES):
        expert_copy(c).wait()


def local(
    mixer_input,
    expert_input,
    gain_mixer,
    gain_expert,
    query_weight,
    key_weight,
    value_weight,
    sink_logits,
    output_weight,
    expert_choice,
    route_weights,
    expert_gate,
    expert_up,
    expert_down,
    shared_gate,
    shared_up,
    shared_down,
):
    tp_count = lax.axis_size("tp")
    ep_count = lax.axis_size("ep")
    tokens, width = expert_input.shape
    own = tokens // tp_count
    top = expert_choice.shape[1]
    local_experts, _, ff = expert_gate.shape
    shared_ff = shared_gate.shape[1]
    experts_all = local_experts * ep_count
    capacity = -(-(2 * own * top // experts_all) // 16) * 16
    slots = experts_all * capacity
    side_rows = slots // 2
    assert tp_count == 4 and local_experts == 1 and ep_count % 4 == 0
    heads = query_weight.shape[1] // HEAD_DIM
    assert heads % 2 == 0 and key_weight.shape[1] == HEAD_DIM and own % WINDOW == 0
    hbm_spec = pl.BlockSpec(memory_space=pltpu.HBM)
    dma = pltpu.SemaphoreType.DMA
    vmem = pltpu.VMEM
    piece = width // PIECES
    count = 4 + PIECES
    scratch = [
        vmem((tokens, width), bf16),
        vmem((tokens, width), bf16),
        vmem((1, width), f32),
        vmem((top, tokens), jnp.int32),
        vmem((top, tokens), f32),
        vmem((tp_count, 4, width, ff // 2), bf16),
        vmem((PIECES, tp_count * ff, piece), bf16),
        vmem((width, shared_ff), bf16),
        vmem((width, shared_ff), bf16),
        vmem((2, tp_count * shared_ff, width // 2), bf16),
        vmem((tokens, width), bf16),
        vmem((1, width), f32),
        vmem(query_weight.shape, bf16),
        vmem((HEAD_DIM, width), bf16),
        vmem((HEAD_DIM, width), bf16),
        vmem(output_weight.shape, bf16),
        vmem((1, heads), f32),
        vmem((heads * WINDOW, 2 * HEAD_DIM), f32),
        vmem((1, 2 * HEAD_DIM), f32),
        vmem((tokens, 2 * HEAD_DIM), f32),
        vmem((tokens, 2 * HEAD_DIM), f32),
        vmem((tokens, heads * HEAD_DIM), bf16),
        vmem((2, WINDOW + tokens, 2 * HEAD_DIM), bf16),
        vmem((tokens, heads * HEAD_DIM), bf16),
        vmem((own, width), bf16),
        vmem((slots, width), bf16),
        vmem((slots, width), bf16),
        vmem((slots, tp_count * ff), bf16),
        vmem((PIECES, slots, piece), bf16),
        vmem((PIECES, slots + side_rows, piece), bf16),
        vmem((top, own, slots), bf16),
        vmem((top, own, own), f32),
        vmem((top, tokens), jnp.int32),
        vmem((top, tokens), f32),
        vmem((top, own, side_rows), bf16),
        vmem((top, own, own), f32),
        vmem((PIECES, own, piece), bf16),
        vmem((PIECES, own, piece), bf16),
        vmem((own, width), f32),
        vmem((own, width), bf16),
        vmem((PIECES, own, piece), bf16),
        dma((1 + PIECES,)),
        vmem((2, 2, own, width), bf16),
        vmem((tokens, shared_ff), bf16),
        vmem((own, tp_count * shared_ff), bf16),
        vmem((2, own, width), bf16),
        vmem((own, width), bf16),
        vmem((own, width), bf16),
        vmem((own, width), bf16),
        vmem((side_rows, width), bf16),
        dma((20 + PIECES,)),
        dma((count,)), dma((count,)),
        dma((count,)), dma((count,)),
        dma((count,)), dma((count,)),
        dma((ep_count,)), dma((ep_count,)),
        dma((ep_count, PIECES)), dma((ep_count + ep_count // 2, PIECES)),
        dma, dma,
        dma, dma,
        dma, dma,
        dma((2,)), dma((2,)),
        dma((PIECES,)), dma((PIECES,)),
        dma((ep_count // 2,)), dma, dma,
        dma((3,)), dma((3,)),
        dma((6,)), dma((6,)),
    ]
    sums = pl.pallas_call(
        functools.partial(mixture_kernel, capacity),
        out_shape=(jax.ShapeDtypeStruct((own, width), bf16),) * 2,
        in_specs=[hbm_spec] * 18,
        out_specs=(hbm_spec,) * 2,
        scratch_shapes=scratch,
        compiler_params=pltpu.CompilerParams(
            collective_id=0, has_side_effects=True, vmem_limit_bytes=62 * 1024 * 1024
        ),
    )(
        expert_input, gain_expert[None, :], expert_choice.T, route_weights.T,
        expert_gate[0], expert_up[0], expert_down[0], shared_gate, shared_up, shared_down,
        mixer_input, gain_mixer[None, :], query_weight, key_weight.T, value_weight.T, output_weight,
        sink_logits[None, :], frequencies(HEAD_DIM),
    )
    def round_both(a_ref, b_ref, mixer_out, expert_out):
        mixer_out[...] = a_ref[...]
        expert_out[...] = b_ref[...]

    return pl.pallas_call(
        round_both,
        grid=(1,),
        out_shape=(jax.ShapeDtypeStruct((own, width), bf16),) * 2,
        in_specs=(pl.BlockSpec((own, width), lambda i: (i, 0)),) * 2,
        out_specs=(pl.BlockSpec((own, width), lambda i: (i, 0)),) * 2,
    )(*sums)


def solution(mesh):
    placed = (
        P("ep", None),
        P("ep", None),
        P(),
        P(),
        P(None, "tp"),
        P(None, "tp"),
        P(None, "tp"),
        P("tp"),
        P("tp", None),
        P("ep", None),
        P("ep", None),
        P("ep", None, "tp"),
        P("ep", None, "tp"),
        P("ep", "tp", None),
        P(None, "tp"),
        P(None, "tp"),
        P("tp", None),
    )
    return jax.shard_map(
        local,
        mesh=mesh,
        in_specs=placed,
        out_specs=(P(("ep", "tp"), None), P(("ep", "tp"), None)),
        check_vma=False,
    )
```

```python
import functools

import jax
import jax.numpy as jnp
import numpy as np
from jax import lax
from jax.experimental import pallas as pl
from jax.experimental.pallas import tpu as pltpu
from jax.sharding import PartitionSpec as P

HEAD_DIM = 64
WINDOW = 128
SEQS = 1
PIECES = 8
BLOCKS = 4
LAG = 2
EARLY = 6

norm_eps = 1e-06
rope_base = 500000.0
bf16 = jnp.bfloat16
f32 = jnp.float32
MESH = pl.DeviceIdType.MESH


def frequencies(head_size):
    half_steps = np.arange(head_size // 2, dtype=np.float64)
    return np.tile(rope_base ** (-(2.0 * half_steps) / head_size), 4).astype(np.float32)[None, :]


def rows_at(start, count, unit):
    return pl.ds(pl.multiple_of(start, unit), count)


def norm_into(target, source, to, start, count, gain):
    step = 32

    def body(i, carry):
        widened = source[rows_at(start + i * step, step, step), :].astype(f32)
        scale = lax.rsqrt(jnp.mean(widened * widened, axis=-1, keepdims=True) + norm_eps)
        target[rows_at(to + i * step, step, step), :] = (widened * scale * gain[...]).astype(bf16)
        return carry

    lax.fori_loop(0, count // step, body, 0)


def silu_times(gate, up):
    return gate / (1.0 + jnp.exp(-gate)) * up


def mixture_kernel(
    capacity,
    x_ref, gain_ref, choice_ref, route_ref,
    wg_ref, wu_ref, wd_ref, sg_ref, su_ref, sd_ref,
    mx_ref, mgain_ref, wq_ref, wk_ref, wv_ref, wo_ref, sink_ref, freq_ref,
    mixer_ref, expert_ref,
    rows_in, normed, gain, choice, route, wgu, wd, sg, su, sd,
    mixer_in, mixer_gain, wq, wk, wv, wo, sink, sunk, freq, cosines, sines, queries, band, attended,
    own_rows, slots_out, slots_in, hidden, result, back, picks, weights_col,
    mirror_choice, mirror_route, mirror_picks, mirror_weights, dense_out, dense_in, expert_sum, mixer_out, expert_out, out_sem,
    mixer_part, shared_hidden, shared_all, half_in, half_out, last_in, mirror_rows, mirror_slots,
    load_sem, far_send, far_recv, mate_send, mate_recv, pass_send, pass_recv,
    slot_send, slot_recv, back_send, back_recv, half_send, half_recv, last_send, last_recv,
    halo_send, halo_recv, mirror_send, mirror_recv, dense_send, dense_recv,
    dealt_send, row_send, row_recv, hid_send, hid_recv, sd_send, sd_recv,
):
    ep_count = lax.axis_size("ep")
    me = lax.axis_index("ep")
    t = lax.axis_index("tp")
    parity = t % 2
    level = t // 2
    mate = t + 1 - 2 * parity
    far = (t + 2) % 4
    far_mate = (mate + 2) % 4
    tokens, width = rows_in.shape
    own = own_rows.shape[0]
    quarter_size = ep_count // 4
    quarter = me // quarter_size
    seat = me % quarter_size
    high = quarter // 2
    middle_one = (quarter + high) % 2
    mirror = (3 - quarter) * quarter_size + seat
    side_rows = 2 * quarter_size * capacity
    ff = wd_ref.shape[0]
    shared_ff = sd_ref.shape[0]
    block = width // BLOCKS
    slots = slots_out.shape[0]
    piece = width // PIECES

    barrier = pltpu.get_barrier_semaphore()

    def greet(k, carry):
        pl.semaphore_signal(barrier, inc=1, device_id={"ep": (me + k) % ep_count}, device_id_type=MESH)
        return carry

    lax.fori_loop(1, ep_count, greet, 0)
    for other in (mate, far, far_mate):
        pl.semaphore_signal(barrier, inc=1, device_id={"tp": other}, device_id_type=MESH)

    part = ff // 2
    halves = [pl.ds(h * part, part) for h in range(2)]
    gate_up_sources = [ref.at[:, half] for half in halves for ref in (wg_ref, wu_ref)]
    sources = gate_up_sources + [wd_ref.at[:, pl.ds(c * piece, piece)] for c in range(PIECES)]

    def gate_up_views(owner):
        return [wgu.at[owner, i] for i in range(4)]

    wide = width // 2

    def sd_view(owner, half):
        return sd.at[half, rows_at(owner * shared_ff, shared_ff, shared_ff)]

    def block_views(owner):
        return gate_up_views(owner) + [wd.at[c, rows_at(owner * ff, ff, ff)] for c in range(PIECES)]

    loads = [
        (gain_ref, gain), (choice_ref, choice), (route_ref, route), (x_ref, rows_in),
        (mgain_ref, mixer_gain), (freq_ref, freq), (mx_ref, mixer_in), (wk_ref, wk), (wv_ref, wv),
        (wq_ref, wq), (sink_ref, sink), (sg_ref, sg), (su_ref, su), (wo_ref, wo),
    ]
    loads += [(sd_ref.at[:, pl.ds(h * wide, wide)], sd_view(t, h)) for h in range(2)]
    loads += list(zip(sources, block_views(t)))
    loads = [pltpu.make_async_copy(a, b, load_sem.at[i]) for i, (a, b) in enumerate(loads)]
    for load in loads:
        load.start()

    pl.semaphore_wait(barrier, ep_count + 2)

    def remote(src, dst, send, recv, device):
        return pltpu.make_async_remote_copy(
            src_ref=src, dst_ref=dst, send_sem=send, recv_sem=recv,
            device_id=device, device_id_type=MESH,
        )

    def views_copy(srcs, owner, send, recv, device):
        return [
            remote(a, b, send.at[i], recv.at[i], device)
            for i, (a, b) in enumerate(zip(srcs, block_views(owner)))
        ]

    to_far = views_copy(sources, t, far_send, far_recv, {"tp": far})
    to_mate = views_copy(sources, t, mate_send, mate_recv, {"tp": mate})
    from_far = views_copy(sources, far, far_send, far_recv, {"tp": far})
    from_mate = views_copy(sources, mate, mate_send, mate_recv, {"tp": mate})
    to_pass = views_copy(block_views(far), far, pass_send, pass_recv, {"tp": mate})
    from_pass = views_copy(block_views(far), far_mate, pass_send, pass_recv, {"tp": mate})
    side_bit = me % 2
    beside = me + 1 - 2 * side_bit
    sd_to_far = remote(
        sd_ref.at[:, rows_at(side_bit * wide, wide, wide)], sd_view(t, side_bit),
        sd_send.at[0], sd_recv.at[0], {"tp": far},
    )
    sd_from_far = remote(sd_view(far, side_bit), sd_view(far, side_bit), sd_send.at[0], sd_recv.at[0], {"tp": far})
    sd_to_beside = remote(sd_view(far, side_bit), sd_view(far, side_bit), sd_send.at[1], sd_recv.at[1], {"ep": beside})
    sd_from_beside = remote(sd_view(far, 1 - side_bit), sd_view(far, 1 - side_bit), sd_send.at[1], sd_recv.at[1], {"ep": beside})
    sd_to_mate, sd_from_mate = (
        [
            remote(sd_ref.at[:, pl.ds(h * wide, wide)], sd_view(owner, h), sd_send.at[4 + h], sd_recv.at[4 + h], {"tp": mate})
            for h in range(2)
        ]
        for owner in (t, mate)
    )
    sd_passed = [
        (
            remote(sd_view(far, half), sd_view(far, half), sd_send.at[2 + i], sd_recv.at[2 + i], {"tp": mate}),
            remote(sd_view(far_mate, half), sd_view(far_mate, half), sd_send.at[2 + i], sd_recv.at[2 + i], {"tp": mate}),
        )
        for i, half in enumerate((side_bit, 1 - side_bit))
    ]
    for copy in to_far[: 4 + EARLY]:
        copy.start()
    sd_to_far.start()
    for copy in to_far[4 + EARLY :]:
        copy.start()

    for i in (0, 1, 2, 3):
        loads[i].wait()
    mirrored = [
        remote(a, b, mirror_send.at[i], mirror_recv.at[i], {"ep": mirror})
        for i, (a, b) in enumerate(((choice, mirror_choice), (route, mirror_route)))
    ]

    @pl.when(middle_one == 1)
    def _():
        for copy in mirrored:
            copy.start()

    norm_into(own_rows, rows_in, 0, t * own, own, gain)
    lanes = rows_at(t * own, own, own)
    top = choice.shape[0]
    row_ids = lax.broadcasted_iota(jnp.int32, (slots // capacity, own), 0)
    earlier = lax.broadcasted_iota(jnp.int32, (own, own), 0)
    later = lax.broadcasted_iota(jnp.int32, (own, own), 1)
    before = (earlier < later).astype(f32)

    def slots_of(choices):
        chosen = choices[:, lanes]
        named = [row_ids == chosen[k : k + 1, :] for k in range(top)]
        named_any = functools.reduce(jnp.logical_or, named).astype(f32)
        ranks = jnp.dot(named_any, before, preferred_element_type=f32)
        return [
            chosen[k : k + 1, :] * capacity
            + jnp.sum(jnp.where(named[k], ranks, 0.0), axis=0, keepdims=True).astype(jnp.int32)
            for k in range(top)
        ]

    def column_of(row):
        return jnp.broadcast_to(row.astype(f32), (own, own)).T

    slot_rows = slots_of(choice)
    slot_ids = lax.broadcasted_iota(jnp.int32, (slots, own), 0)
    spread = functools.reduce(jnp.logical_or, [slot_ids == row for row in slot_rows])
    spread = spread.astype(f32).astype(bf16)
    for c in range(BLOCKS):
        cols = pl.ds(c * block, block)
        slots_out[:, cols] = jnp.dot(spread, own_rows[:, cols], preferred_element_type=f32).astype(bf16)

    def slot_block(ref, owner):
        return ref.at[rows_at(owner * capacity, capacity, capacity)]

    def slot_copy(k, target, origin):
        return remote(
            slot_block(slots_out, target), slot_block(slots_in, origin),
            slot_send.at[k], slot_recv.at[k], {"ep": target},
        )

    rows_copy = remote(own_rows, mirror_rows, row_send, row_recv, {"ep": mirror})

    def send_slots(side, k):
        target = (me + k) % ep_count

        @pl.when(target // (2 * quarter_size) == side)
        def _():
            slot_copy(k, target, me).start()

    def send_near(k, carry):
        send_slots(high, k)
        return carry

    def send_far(k, carry):
        send_slots(1 - high, k)
        return carry

    lax.fori_loop(1, ep_count, send_near, 0)

    for i in range(4, 9):
        loads[i].wait()
    pair = 2 * HEAD_DIM
    lane = lax.broadcasted_iota(jnp.int32, (1, pair), 1)
    first_half = lane % HEAD_DIM < HEAD_DIM // 2
    lower = lane < HEAD_DIM
    twice = lax.broadcasted_iota(jnp.int32, (HEAD_DIM, pair), 0)
    twice = (lax.broadcasted_iota(jnp.int32, (HEAD_DIM, pair), 1) % HEAD_DIM == twice).astype(f32).astype(bf16)
    first_position = me % (ep_count // SEQS) * tokens
    transposed = (((1,), (1,)), ((), ()))

    def turn(heads, rows):
        swapped = jnp.where(
            first_half,
            pltpu.roll(heads, pair - HEAD_DIM // 2, 1),
            pltpu.roll(heads, HEAD_DIM // 2, 1),
        )
        return heads * cosines[rows, :] + swapped * sines[rows, :]

    def project_keys(i, carry):
        rows = rows_at(i * WINDOW, WINDOW, WINDOW)
        after = rows_at((i + 1) * WINDOW, WINDOW, WINDOW)
        norm_into(normed, mixer_in, i * WINDOW, i * WINDOW, WINDOW, mixer_gain)
        position = lax.broadcasted_iota(jnp.int32, (WINDOW, pair), 0) + (first_position + i * WINDOW)
        angles = position.astype(f32) * freq[...]
        sine = jnp.sin(angles)
        cosines[rows, :] = jnp.cos(angles)
        sines[rows, :] = jnp.where(first_half, -sine, sine)
        source = normed[rows, :]
        keys = lax.dot_general(source, wk[...], transposed, preferred_element_type=f32).astype(bf16)
        keys = jnp.dot(keys, twice, preferred_element_type=f32)
        band[0, after, :] = turn(keys, rows).astype(bf16)
        values = lax.dot_general(source, wv[...], transposed, preferred_element_type=f32).astype(bf16)
        band[1, after, :] = jnp.dot(values, twice, preferred_element_type=f32).astype(bf16)
        return carry

    def halo_copy(target):
        return remote(
            band.at[:, pl.ds(tokens, WINDOW)], band.at[:, pl.ds(0, WINDOW)],
            halo_send, halo_recv, {"ep": target},
        )

    last_block = tokens // WINDOW - 1
    project_keys(last_block, 0)
    halo_copy((me + 1) % ep_count).start()

    @pl.when(middle_one == 1)
    def _():
        rows_copy.start()

    for copy in to_mate + sd_to_mate:
        copy.start()

    own_block = rows_at(me * capacity, capacity, capacity)
    slots_in[own_block, :] = slots_out[own_block, :]
    lane_ids = lax.broadcasted_iota(jnp.int32, (own, slots), 1)
    for k in range(top):
        picks[k] = (lane_ids == column_of(slot_rows[k])[:, :1].astype(jnp.int32)).astype(f32).astype(bf16)
        weights_col[k] = column_of(route[k : k + 1, lanes])

    @pl.when(middle_one == 1)
    def _():
        for c in range(PIECES):
            back[c, rows_at((1 - high) * side_rows, side_rows, capacity), :] = jnp.zeros((side_rows, piece), bf16)

    @pl.when(middle_one == 0)
    def _():
        dense_in[...] = jnp.zeros(dense_in.shape, bf16)

    half_copy = remote(mixer_part.at[1 - parity], half_in, half_send, half_recv, {"tp": mate})
    last_copy = remote(half_out, last_in, last_send, last_recv, {"tp": far})

    lax.fori_loop(0, last_block, project_keys, 0)
    loads[9].wait()
    pairs = wq.shape[1] // pair

    def project(i, carry):
        rows = rows_at(i * WINDOW, WINDOW, WINDOW)
        for j in range(pairs):
            cols = pl.ds(j * pair, pair)
            heads = jnp.dot(normed[rows, :], wq[:, cols], preferred_element_type=f32)
            turned_heads = turn(heads.astype(bf16).astype(f32), rows).astype(bf16)
            queries[rows, cols] = (turned_heads.astype(f32) * HEAD_DIM ** -0.5).astype(bf16)
        return carry

    lax.fori_loop(0, tokens // WINDOW, project, 0)

    norm_into(normed, rows_in, 0, 0, tokens, gain)
    for i in (11, 12):
        loads[i].wait()
    for r in range(2):
        rows = pl.ds(r * (tokens // 2), tokens // 2)
        gate = jnp.dot(normed[rows, :], sg[...], preferred_element_type=f32)
        up = jnp.dot(normed[rows, :], su[...], preferred_element_type=f32)
        shared_hidden[rows, :] = silu_times(gate, up).astype(bf16)

    def hid_copy(i, device, origin):
        return remote(
            shared_hidden.at[rows_at(device * own, own, own)],
            shared_all.at[:, rows_at(origin * shared_ff, shared_ff, shared_ff)],
            hid_send.at[i], hid_recv.at[i], {"tp": device},
        )

    hid_out = [hid_copy(i, device, t) for i, device in enumerate((mate, far, far_mate))]
    hid_in = [hid_copy(i, device, device) for i, device in enumerate((mate, far, far_mate))]
    for copy in hid_out:
        copy.start()
    shared_all[:, rows_at(t * shared_ff, shared_ff, shared_ff)] = shared_hidden[rows_at(t * own, own, own), :]

    @pl.when(middle_one == 0)
    def _():
        lax.fori_loop(1, ep_count, send_far, 0)

    for i in (10, 13):
        loads[i].wait()
    halo_copy((me + 1) % ep_count).wait_recv()
    count = 2 * pairs
    row = lax.broadcasted_iota(jnp.int32, (WINDOW, 2 * WINDOW), 0)
    key = lax.broadcasted_iota(jnp.int32, (WINDOW, 2 * WINDOW), 1)
    distance = row + WINDOW - key
    in_window = (distance >= 0) & (distance < WINDOW)

    for head in range(count):
        sunk[pl.ds(head * WINDOW, WINDOW), :] = jnp.broadcast_to(sink[:, head : head + 1], (WINDOW, pair))

    def attend(i, carry):
        rows = rows_at(i * WINDOW, WINDOW, WINDOW)
        reach = rows_at(i * WINDOW, 2 * WINDOW, WINDOW)
        allowed = in_window & (key + (first_position + (i - 1) * WINDOW) >= 0)
        both = [queries[rows, pl.ds(j * pair, pair)] for j in range(pairs)]
        none = jnp.zeros((WINDOW, pair), bf16)
        kept = jnp.concatenate(
            [jnp.where(side, heads, none) for heads in both for side in (lower, ~lower)], axis=0
        )
        scores = lax.dot_general(kept, band[0, reach, :], transposed, preferred_element_type=f32)
        scores = jnp.where(allowed[None], scores.reshape(count, WINDOW, 2 * WINDOW), -jnp.inf)
        scores = scores.reshape(count * WINDOW, 2 * WINDOW)
        sinks = sunk[:, :1]
        peak = jnp.maximum(jnp.max(scores, axis=-1, keepdims=True), sinks)
        raised = jnp.exp(scores - peak).astype(bf16)
        values = jnp.concatenate([band[1, reach, :], jnp.ones((2 * WINDOW, pair), bf16)], axis=1)
        mixed = jnp.dot(raised, values, preferred_element_type=f32)
        mixed = (mixed[:, :pair] / (mixed[:, pair:] + jnp.exp(sinks - peak))).reshape(count, WINDOW, pair)
        for j in range(pairs):
            attended[rows, pl.ds(j * pair, pair)] = jnp.where(
                lower, mixed[2 * j], mixed[2 * j + 1]
            ).astype(bf16)
        return carry

    lax.fori_loop(0, tokens // WINDOW, attend, 0)
    for owner in range(4):
        for c in range(BLOCKS):
            cols = pl.ds(c * block, block)
            mixer_part[owner % 2, owner // 2, :, cols] = jnp.dot(
                attended[pl.ds(owner * own, own), :], wo[:, cols], preferred_element_type=f32
            ).astype(bf16)
    half_copy.start()
    def dealt_copy(n):
        target = high * 2 * quarter_size + n
        return remote(
            slot_block(mirror_slots, n), slot_block(slots_in, mirror),
            dealt_send.at[n], slot_recv.at[(target - mirror + ep_count) % ep_count], {"ep": target},
        )

    my_place = (quarter % 2) * quarter_size + seat

    @pl.when(middle_one == 1)
    def _():
        for copy in mirrored:
            copy.wait_recv()
        mirror_slot_rows = slots_of(mirror_choice)
        near_ids = lax.broadcasted_iota(jnp.int32, (own, side_rows), 1) + high * side_rows
        for k, row in enumerate(mirror_slot_rows):
            mirror_picks[k] = (near_ids == column_of(row)[:, :1].astype(jnp.int32)).astype(f32).astype(bf16)
            mirror_weights[k] = column_of(mirror_route[k : k + 1, lanes])
        rows_copy.wait_recv()
        side_ids = lax.broadcasted_iota(jnp.int32, (side_rows, own), 0) + high * side_rows
        spread_side = functools.reduce(jnp.logical_or, [side_ids == row for row in mirror_slot_rows])
        spread_side = spread_side.astype(f32).astype(bf16)
        for c in range(BLOCKS):
            cols = pl.ds(c * block, block)
            mirror_slots[:, cols] = jnp.dot(
                spread_side, mirror_rows[:, cols], preferred_element_type=f32
            ).astype(bf16)

        def deal(n, carry):
            @pl.when(n != my_place)
            def _():
                dealt_copy(n).start()

            return carry

        lax.fori_loop(0, 2 * quarter_size, deal, 0)
        slots_in[rows_at(mirror * capacity, capacity, capacity), :] = mirror_slots[
            rows_at(my_place * capacity, capacity, capacity), :
        ]

    half_copy.wait_recv()
    half_out[...] = (mixer_part[parity, 1 - level].astype(f32) + half_in[1 - level].astype(f32)).astype(bf16)
    last_copy.start()

    def hidden_block(owner, side, half):
        rows = rows_at(side * side_rows, side_rows, capacity)
        weights = jnp.concatenate([wgu[owner, 2 * half], wgu[owner, 2 * half + 1]], axis=1)
        both = jnp.dot(slots_in[rows, :], weights, preferred_element_type=f32)
        hidden[rows, rows_at(owner * ff + half * part, part, part)] = silu_times(
            both[:, :part], both[:, part:]
        ).astype(bf16)

    def pass_on(i):
        from_far[i].wait_recv()
        to_pass[i].start()

    pass_on(0)

    def wait_slots(side):
        def wait_one(k, carry):
            source = (me + ep_count - k) % ep_count

            @pl.when((source // (2 * quarter_size) == side) & (middle_one * (source == mirror) == 0))
            def _():
                slot_copy(k, me, source).wait_recv()

            return carry

        lax.fori_loop(1, ep_count, wait_one, 0)

    wait_slots(high)
    for i in range(14, 20 + PIECES):
        loads[i].wait()
    for half in range(2):
        hidden_block(t, high, half)
    for copy in from_mate:
        copy.wait_recv()
    for half in range(2):
        hidden_block(mate, high, half)
    pass_on(1)
    hidden_block(far, high, 0)
    pass_on(2)
    for i in (0, 1):
        from_pass[i].wait_recv()
    hidden_block(far_mate, high, 0)
    pass_on(3)
    wait_slots(1 - high)
    for half in range(2):
        hidden_block(t, 1 - high, half)
        hidden_block(mate, 1 - high, half)
    hidden_block(far, 1 - high, 0)
    hidden_block(far_mate, 1 - high, 0)
    for side in range(2):
        hidden_block(far, side, 1)
    pass_on(4)
    for i in (2, 3):
        from_pass[i].wait_recv()
    for side in range(2):
        hidden_block(far_mate, side, 1)

    def is_low_middle(q):
        return (q % 2) * (1 - q // 2)

    def is_high_middle(q):
        return (q // 2) * (1 - q % 2)

    def turned(source, target):
        return is_low_middle(target) * (source // 2) + is_high_middle(target) * (1 - source // 2)

    def landing(source, source_seat, target):
        stop = turned(source, target)
        straight = source * quarter_size + source_seat
        return (1 - stop) * straight + stop * (ep_count + (source % 2) * quarter_size + source_seat)

    def back_copy(k, c, owner, target, block):
        cols = pl.ds(c * piece, piece)
        return remote(
            slot_block(result.at[c], owner), slot_block(back.at[c], block),
            back_send.at[k, c], back_recv.at[block, c], {"ep": target},
        )

    def each_back(c, remote_do, local_do):
        for n, q in enumerate((1, 0, 2, 3)):
            target = high * q + (1 - high) * (3 - q)
            stop = turned(quarter, target)
            via = target + stop * (2 * high - 1)

            def step(j, carry, n=n, target=target, via=via):
                to_seat = (seat + j) % quarter_size
                owner = target * quarter_size + to_seat
                device = via * quarter_size + to_seat
                block = landing(quarter, seat, target)

                @pl.when(device != me)
                def _():
                    remote_do(back_copy(n * quarter_size + j, c, owner, device, block))

                if local_do is not None:
                    @pl.when(device == me)
                    def _():
                        local_do(owner, block)

                return carry

            lax.fori_loop(0, quarter_size, step, 0)

    def wait_block(c, block):
        back_copy(0, c, me, me, block).wait_recv()

    def dense_copy(c):
        cols = pl.ds(c * piece, piece)
        return remote(
            dense_out.at[c], dense_in.at[c], dense_send.at[c], dense_recv.at[c], {"ep": mirror}
        )

    def relay(c):
        cols = pl.ds(c * piece, piece)

        @pl.when(middle_one == 1)
        def _():
            def wait_relayed(n, carry):
                @pl.when(n != (quarter % 2) * quarter_size + seat)
                def _():
                    wait_block(c, ep_count + n)

                return carry

            lax.fori_loop(0, 2 * quarter_size, wait_relayed, 0)
            total = 0.0
            for k in range(top):
                total = total + mirror_weights[k][:, :1] * jnp.dot(
                    mirror_picks[k], back[c, pl.ds(slots, side_rows), :], preferred_element_type=f32
                )
            dense_out[c] = total.astype(bf16)
            dense_copy(c).start()

    for c in range(PIECES):
        cols = pl.ds(c * piece, piece)
        from_pass[4 + c].wait_recv()
        result[c] = jnp.dot(hidden[...], wd[c], preferred_element_type=f32).astype(bf16)

        def keep(owner, block, c=c):
            back[c, rows_at(block * capacity, capacity, capacity), :] = result[
                c, rows_at(owner * capacity, capacity, capacity), :
            ]

        each_back(c, lambda copy: copy.start(), keep)
        if c + 1 == EARLY:
            sd_from_far.wait_recv()
            sd_to_beside.start()
            sd_passed[0][0].start()
        if c + 1 < PIECES:
            pass_on(5 + c)
        if c >= LAG:
            relay(c - LAG)
    for copy in to_far + to_mate + to_pass + hid_out + sd_to_mate:
        copy.wait_send()
    for copy in (sd_to_far, sd_to_beside, sd_passed[0][0], half_copy):
        copy.wait_send()

    @pl.when(middle_one == 1)
    def _():
        rows_copy.wait_send()
        for copy in mirrored:
            copy.wait_send()

        def dealt_done(n, carry):
            @pl.when(n != my_place)
            def _():
                dealt_copy(n).wait_send()

            return carry

        lax.fori_loop(0, 2 * quarter_size, dealt_done, 0)

    halo_copy((me + 1) % ep_count).wait_send()

    def drain(k, carry):
        target = (me + k) % ep_count
        other = target // (2 * quarter_size)

        @pl.when(middle_one * (other + high - 2 * other * high) == 0)
        def _():
            slot_copy(k, target, me).wait_send()

        return carry

    lax.fori_loop(1, ep_count, drain, 0)

    def back_done(c):
        each_back(c, lambda copy: copy.wait_send(), None)

        @pl.when(middle_one == 1)
        def _():
            dense_copy(c).wait_send()

    sd_from_beside.wait_recv()
    sd_passed[1][0].start()
    for c in range(PIECES - LAG, PIECES):
        relay(c)
    for copy in hid_in + sd_from_mate + [sd_passed[0][1]]:
        copy.wait_recv()
    sd_passed[1][1].wait_recv()
    for c in range(BLOCKS):
        cols = pl.ds(c * block, block)
        expert_sum[:, cols] = jnp.dot(shared_all[...], sd[c // (BLOCKS // 2), :, pl.ds(c % (BLOCKS // 2) * block, block)], preferred_element_type=f32)

    mixer_copy = pltpu.make_async_copy(mixer_out, mixer_ref, out_sem.at[PIECES])

    def expert_copy(c):
        return pltpu.make_async_copy(
            expert_out.at[c], expert_ref.at[:, pl.ds(c * piece, piece)], out_sem.at[c]
        )

    for c in range(PIECES):
        cols = pl.ds(c * piece, piece)

        def wait_back(k, carry, c=c):
            source = (me + ep_count - k) % ep_count

            @pl.when(turned(source // quarter_size, quarter) == 0)
            def _():
                wait_block(c, source)

            return carry

        lax.fori_loop(1, ep_count, wait_back, 0)

        @pl.when(middle_one == 1)
        def _(c=c):
            dense_copy(c).wait_recv()

        total = expert_sum[:, cols] + dense_in[c].astype(f32)
        for k in range(top):
            total = total + weights_col[k][:, :1] * jnp.dot(
                picks[k], back[c, pl.ds(0, slots), :], preferred_element_type=f32
            )
        expert_out[c] = total.astype(bf16)
        expert_copy(c).start()
        if c == PIECES - 2:
            last_copy.wait_recv()
            mixer_sum = mixer_part[parity, level].astype(f32) + half_in[level].astype(f32)
            mixer_out[...] = (mixer_sum + last_in[...].astype(f32)).astype(bf16)
            mixer_copy.start()
        if c >= LAG:
            back_done(c - LAG)

    sd_passed[1][0].wait_send()
    last_copy.wait_send()
    for c in range(PIECES - LAG, PIECES):
        back_done(c)
    mixer_copy.wait()
    for c in range(PIECES):
        expert_copy(c).wait()


def local(
    mixer_input,
    expert_input,
    gain_mixer,
    gain_expert,
    query_weight,
    key_weight,
    value_weight,
    sink_logits,
    output_weight,
    expert_choice,
    route_weights,
    expert_gate,
    expert_up,
    expert_down,
    shared_gate,
    shared_up,
    shared_down,
):
    tp_count = lax.axis_size("tp")
    ep_count = lax.axis_size("ep")
    tokens, width = expert_input.shape
    own = tokens // tp_count
    top = expert_choice.shape[1]
    local_experts, _, ff = expert_gate.shape
    shared_ff = shared_gate.shape[1]
    experts_all = local_experts * ep_count
    capacity = -(-(2 * own * top // experts_all) // 16) * 16
    slots = experts_all * capacity
    side_rows = slots // 2
    assert tp_count == 4 and local_experts == 1 and ep_count % 4 == 0
    heads = query_weight.shape[1] // HEAD_DIM
    assert heads % 2 == 0 and key_weight.shape[1] == HEAD_DIM and own % WINDOW == 0
    hbm_spec = pl.BlockSpec(memory_space=pltpu.HBM)
    dma = pltpu.SemaphoreType.DMA
    vmem = pltpu.VMEM
    piece = width // PIECES
    count = 4 + PIECES
    scratch = [
        vmem((tokens, width), bf16),
        vmem((tokens, width), bf16),
        vmem((1, width), f32),
        vmem((top, tokens), jnp.int32),
        vmem((top, tokens), f32),
        vmem((tp_count, 4, width, ff // 2), bf16),
        vmem((PIECES, tp_count * ff, piece), bf16),
        vmem((width, shared_ff), bf16),
        vmem((width, shared_ff), bf16),
        vmem((2, tp_count * shared_ff, width // 2), bf16),
        vmem((tokens, width), bf16),
        vmem((1, width), f32),
        vmem(query_weight.shape, bf16),
        vmem((HEAD_DIM, width), bf16),
        vmem((HEAD_DIM, width), bf16),
        vmem(output_weight.shape, bf16),
        vmem((1, heads), f32),
        vmem((heads * WINDOW, 2 * HEAD_DIM), f32),
        vmem((1, 2 * HEAD_DIM), f32),
        vmem((tokens, 2 * HEAD_DIM), f32),
        vmem((tokens, 2 * HEAD_DIM), f32),
        vmem((tokens, heads * HEAD_DIM), bf16),
        vmem((2, WINDOW + tokens, 2 * HEAD_DIM), bf16),
        vmem((tokens, heads * HEAD_DIM), bf16),
        vmem((own, width), bf16),
        vmem((slots, width), bf16),
        vmem((slots, width), bf16),
        vmem((slots, tp_count * ff), bf16),
        vmem((PIECES, slots, piece), bf16),
        vmem((PIECES, slots + side_rows, piece), bf16),
        vmem((top, own, slots), bf16),
        vmem((top, own, own), f32),
        vmem((top, tokens), jnp.int32),
        vmem((top, tokens), f32),
        vmem((top, own, side_rows), bf16),
        vmem((top, own, own), f32),
        vmem((PIECES, own, piece), bf16),
        vmem((PIECES, own, piece), bf16),
        vmem((own, width), f32),
        vmem((own, width), bf16),
        vmem((PIECES, own, piece), bf16),
        dma((1 + PIECES,)),
        vmem((2, 2, own, width), bf16),
        vmem((tokens, shared_ff), bf16),
        vmem((own, tp_count * shared_ff), bf16),
        vmem((2, own, width), bf16),
        vmem((own, width), bf16),
        vmem((own, width), bf16),
        vmem((own, width), bf16),
        vmem((side_rows, width), bf16),
        dma((20 + PIECES,)),
        dma((count,)), dma((count,)),
        dma((count,)), dma((count,)),
        dma((count,)), dma((count,)),
        dma((ep_count,)), dma((ep_count,)),
        dma((ep_count, PIECES)), dma((ep_count + ep_count // 2, PIECES)),
        dma, dma,
        dma, dma,
        dma, dma,
        dma((2,)), dma((2,)),
        dma((PIECES,)), dma((PIECES,)),
        dma((ep_count // 2,)), dma, dma,
        dma((3,)), dma((3,)),
        dma((6,)), dma((6,)),
    ]
    sums = pl.pallas_call(
        functools.partial(mixture_kernel, capacity),
        out_shape=(jax.ShapeDtypeStruct((own, width), bf16),) * 2,
        in_specs=[hbm_spec] * 18,
        out_specs=(hbm_spec,) * 2,
        scratch_shapes=scratch,
        compiler_params=pltpu.CompilerParams(
            collective_id=0, has_side_effects=True, vmem_limit_bytes=62 * 1024 * 1024
        ),
    )(
        expert_input, gain_expert[None, :], expert_choice.T, route_weights.T,
        expert_gate[0], expert_up[0], expert_down[0], shared_gate, shared_up, shared_down,
        mixer_input, gain_mixer[None, :], query_weight, key_weight.T, value_weight.T, output_weight,
        sink_logits[None, :], frequencies(HEAD_DIM),
    )
    def round_both(a_ref, b_ref, mixer_out, expert_out):
        mixer_out[...] = a_ref[...]
        expert_out[...] = b_ref[...]

    return pl.pallas_call(
        round_both,
        grid=(1,),
        out_shape=(jax.ShapeDtypeStruct((own, width), bf16),) * 2,
        in_specs=(pl.BlockSpec((own, width), lambda i: (i, 0)),) * 2,
        out_specs=(pl.BlockSpec((own, width), lambda i: (i, 0)),) * 2,
    )(*sums)


def solution(mesh):
    placed = (
        P("ep", None),
        P("ep", None),
        P(),
        P(),
        P(None, "tp"),
        P(None, "tp"),
        P(None, "tp"),
        P("tp"),
        P("tp", None),
        P("ep", None),
        P("ep", None),
        P("ep", None, "tp"),
        P("ep", None, "tp"),
        P("ep", "tp", None),
        P(None, "tp"),
        P(None, "tp"),
        P("tp", None),
    )
    return jax.shard_map(
        local,
        mesh=mesh,
        in_specs=placed,
        out_specs=(P(("ep", "tp"), None), P(("ep", "tp"), None)),
        check_vma=False,
    )
```
